256 devices in a mesh: ep: 64 (over z, x, core), tp: 4 (over y).
Axes of the slice: x: 4, y: 4, z: 8, core: 2. Of those that a mesh axis runs over, the one named last changes fastest.
Arguments:
- recurrence_query: bfloat16 [8192, 1024], P('ep', 'tp'), may hold values from -6 to 6
- forget_preactivation: bfloat16 [8192, 1024], P('ep', 'tp'), may hold values from -7 to 7
- recurrence_value: bfloat16 [8192, 1024], P('ep', 'tp'), may hold values from -6 to 6
- output_gate_preactivation: bfloat16 [8192, 1024], P('ep', 'tp'), may hold values from -6 to 6
- forget_margin: float32 [1024], P('tp'), may hold values from 0 to 0.1
- surge_log_decay: float32 [8, 8192], P('tp', 'ep'), may hold values from -1.4 to 0
- head_norm_gain: float32 [1024], P('tp'), may hold values from 0.1 to 1.9
- recurrence_output_matrix: bfloat16 [1024, 4096], P('tp'), may hold values from -0.1875 to 0.1875
- second_micro_input: bfloat16 [8192, 4096], P(('ep', 'tp')), may hold values from -6 to 6
- expert_norm_gain: float32 [4096], replicated, may hold values from 0.1 to 1.9
- routes: int32 [8192, 2], P('ep'), may hold values from 0 to 63, all different within a row; in each aligned block of 32 rows (0 to 31, 32 to 63, ...) at most 2 rows name the same one
- router_chosen_logits: float32 [8192, 2], P(('ep', 'tp')), may hold values from -6 to 6
- expert_gate_matrix: bfloat16 [64, 4096, 1408], P('ep', None, 'tp'), may hold values from -0.09375 to 0.09375
- expert_up_matrix: bfloat16 [64, 4096, 1408], P('ep', None, 'tp'), may hold values from -0.09375 to 0.09375
- expert_down_matrix: bfloat16 [64, 1408, 4096], P('ep', 'tp'), may hold values from -0.15625 to 0.15625
Outputs:
- mixed: bfloat16 [8192, 4096], P(('ep', 'tp'))
- moe_out: bfloat16 [8192, 4096], P(('ep', 'tp'))
The draws below stay inside these ranges and needn't reach their ends.
Inputs may be any that keep to these rules, and one draw needn't show every extreme that they name: `routes`: in the rows of one device (aligned blocks of 32 rows) no expert is named more than 2 times, and the experts of a row differ.
All inputs are finite; a program needn't handle non-finite values.
Results may differ from the reference program's by a relative error of at most 0.019.
Values may be sent and summed in bfloat16 or wider, within the bound.
A program may use at most 128 MiB of HBM per device.

```python
import math
import jax
import jax.numpy as jnp
import numpy as np
from jax import lax

D = 4096
HEADS = 8
KEY = 128
VAL = 128
FF = 1408
TOP = 2
SPAN = 64
SEQ_DEV = 128
TB_DEV = 32
EXPERTS = 64
CAP = 2
TOKENS_A = 8192
TOKENS_B = 8192
N_EP = 64
N_TP = 4


def draw_forget_preactivation(key, part):
    noise_key, shift_key = jax.random.split(jax.random.fold_in(key, 11))
    blocks = TOKENS_A // SEQ_DEV
    shifts = jax.random.uniform(shift_key, (blocks, 1, HEADS * KEY), jnp.float32, -1.0, 1.0)
    noise = jnp.clip(jax.random.normal(noise_key, (blocks, SEQ_DEV, HEADS * KEY), jnp.float32), -6.0, 6.0)
    return (noise + shifts).reshape(TOKENS_A, HEADS * KEY).astype(jnp.bfloat16)


def draw_forget_margin(key, part):
    pick_key, fast_key, slow_key = jax.random.split(jax.random.fold_in(key, 23), 3)
    share = 0.5
    fast_head = jax.random.uniform(pick_key, (HEADS, 1), jnp.float32) < share
    fast_gap = jnp.exp(jax.random.uniform(fast_key, (HEADS, KEY), jnp.float32, math.log(0.04), math.log(0.1)))
    slow_gap = jnp.exp(jax.random.uniform(slow_key, (HEADS, KEY), jnp.float32, math.log(0.3), math.log(1.5))) / TOKENS_A
    return jnp.where(fast_head, fast_gap, slow_gap).reshape(HEADS * KEY).astype(jnp.float32)


def draw_surge_log_decay(key, part):
    spot_key, depth_key = jax.random.split(jax.random.fold_in(key, 37))
    spots = jax.random.randint(spot_key, (HEADS, 2, 1), 0, TOKENS_A)
    depth = jax.random.uniform(depth_key, (HEADS, 2, 1), jnp.float32, math.log(0.5), math.log(0.8))
    hits = spots == jnp.arange(TOKENS_A, dtype=jnp.int32)[None, None, :]
    return jnp.sum(jnp.where(hits, depth, 0.0), axis=1).astype(jnp.float32)


def block_levels(stream_key, extent, shards, low, high):
    level, own = 1.0, jax.random.fold_in(stream_key, 6)
    for axis_at, parts in shards:
        heights = jnp.exp(jax.random.uniform(jax.random.fold_in(own, axis_at), (parts,), jnp.float32, low / len(shards), high / len(shards)))
        level = level * jnp.repeat(heights, extent[axis_at] // parts).reshape([-1 if axis == axis_at else 1 for axis in range(len(extent))])
    return level


def deal_out(own_key, own, number, rows, amount, top, most, slope):
    order = jax.random.permutation(own_key, amount)
    heavy_load, ordinary = shares(amount, rows * top, most, slope, True), shares(amount, rows * top, most, slope, False)
    places = jnp.arange(amount)

    def named(tallies, turn):
        used = int((tallies > 0).sum())
        fixed = max(1, used // 4)
        passed = fixed + (places - fixed + turn * (used - fixed)) % max(1, amount - fixed)
        return jnp.zeros((amount,), jnp.int32).at[order[jnp.where(places < fixed, places, passed)]].set(jnp.asarray(tallies, jnp.int32))

    tallies = jnp.where(number % 4 == 0, named(heavy_load, number // 4), named(ordinary, number - number // 4 - 1))
    mixed = jax.random.permutation(jax.random.fold_in(own, 3), amount)
    donor, taker = mixed[0:amount // 2 * 2:2], mixed[1:amount // 2 * 2:2]
    margin = jnp.minimum(tallies[donor] - 1, most - tallies[taker]) // 2
    margin = jnp.where((donor == order[0]) | (taker == order[0]) | (tallies[taker] == 0), 0, jnp.maximum(margin, 0))
    passed = jax.random.randint(jax.random.fold_in(own, 4), (amount // 2,), 0, 1 << 20) % (margin + 1)
    tallies = tallies.at[donor].add(-passed).at[taker].add(passed)
    items = jnp.searchsorted(jnp.cumsum(tallies), jnp.arange(rows * top), side="right").astype(jnp.int32)
    grid = items.reshape(top, rows).T
    grid = grid[jax.random.permutation(jax.random.fold_in(own, 1), rows)]
    turn = jax.random.randint(jax.random.fold_in(own, 2), (rows, 1), 0, top)
    return jnp.take_along_axis(grid, (jnp.arange(top)[None, :] + turn) % top, axis=1)


def shares(count, total, bound, slope, full):
    weights = [(1 << 20) // math.isqrt(grade ** slope) + 1 for grade in range(1, count + 1)]
    largest = bound if full else min(bound, max(-(-total // count), total * weights[0] // sum(weights)))
    least = 1 if total - largest >= count - 1 else 0
    holding, surplus = [largest] + [least] * (count - 1), total - largest - least * (count - 1)
    while surplus > 0:
        candidates = [i for i in range(1, count) if holding[i] < largest] or [i for i in range(1, count) if holding[i] < bound]
        whole, remaining = sum([weights[i] for i in candidates]), surplus
        for i in candidates:
            addition = min(bound - holding[i], max(1, remaining * weights[i] // whole), surplus)
            holding[i] = holding[i] + addition
            surplus = surplus - addition
    return np.array(holding)


def normal_values(rng, dims, deviation, reach, shards=(), kind=jnp.bfloat16):
    values = jax.random.normal(rng, dims, jnp.float32) * deviation
    if len(shards) > 0:
        values = block_levels(rng, dims, shards, -0.22, 0.18) * values
    return jnp.clip(values, min=-reach, max=reach).astype(kind)


def setup_inputs(seed: int = 0) -> dict:
    streams_of = jax.random.split(jax.random.key(seed), 16)
    recurrence_query = normal_values(streams_of[0], (TOKENS_A, HEADS * KEY), 1.0, 6.0, ((0, 64), (1, 4)))
    forget_preactivation = draw_forget_preactivation(jax.random.fold_in(streams_of[15], 71), 0)
    recurrence_value = normal_values(streams_of[2], (TOKENS_A, HEADS * VAL), 1.0, 6.0, ((0, 64), (1, 4)))
    output_gate_preactivation = normal_values(streams_of[3], (TOKENS_A, HEADS * VAL), 1.0, 6.0, ((0, 64), (1, 4)))
    forget_margin = draw_forget_margin(jax.random.fold_in(streams_of[15], 71), 0)
    surge_log_decay = draw_surge_log_decay(jax.random.fold_in(streams_of[15], 71), 0)
    head_norm_gain = jnp.clip(1.0 + 0.18 * jax.random.normal(streams_of[6], (HEADS * VAL,), jnp.float32), 0.1, 1.9)
    recurrence_output_matrix = normal_values(streams_of[7], (HEADS * VAL, D), (HEADS * VAL) ** -0.5, 0.1875, ((0, 4),))
    second_micro_input = normal_values(streams_of[8], (TOKENS_B, D), 1.0, 6.0, ((0, 256),))
    expert_norm_gain = jnp.clip(1.0 + 0.18 * jax.random.normal(streams_of[9], (D,), jnp.float32), 0.1, 1.9)
    routes_keys = jax.random.split(jax.random.fold_in(streams_of[10], 1), TOKENS_B // TB_DEV)
    routes_turns = jax.random.permutation(jax.random.fold_in(streams_of[10], 3), TOKENS_B // TB_DEV)
    routes = jax.vmap(lambda own, number: deal_out(jax.random.fold_in(streams_of[10], 2), own, number, TB_DEV, EXPERTS, TOP, CAP, 1))(routes_keys, routes_turns).reshape((TOKENS_B, TOP))
    router_chosen_logits = normal_values(streams_of[11], (TOKENS_B, TOP), 1.0, 6.0, ((0, 256),), jnp.float32)
    expert_gate_matrix = normal_values(streams_of[12], (EXPERTS, D, FF), D ** -0.5, 0.09375, ((0, 64), (2, 4)))
    expert_up_matrix = normal_values(streams_of[13], (EXPERTS, D, FF), D ** -0.5, 0.09375, ((0, 64), (2, 4)))
    expert_down_matrix = normal_values(streams_of[14], (EXPERTS, FF, D), FF ** -0.5, 0.15625, ((0, 64), (1, 4)))
    return {"recurrence_query": recurrence_query, "forget_preactivation": forget_preactivation, "recurrence_value": recurrence_value, "output_gate_preactivation": output_gate_preactivation, "forget_margin": forget_margin, "surge_log_decay": surge_log_decay, "head_norm_gain": head_norm_gain, "recurrence_output_matrix": recurrence_output_matrix, "second_micro_input": second_micro_input, "expert_norm_gain": expert_norm_gain, "routes": routes, "router_chosen_logits": router_chosen_logits, "expert_gate_matrix": expert_gate_matrix, "expert_up_matrix": expert_up_matrix, "expert_down_matrix": expert_down_matrix}


epsilon = 1e-06
highest = lax.Precision.HIGHEST

def span_recurrence(query, inflow, decay_logarithm, values):
    number_of_heads, seq_len, key_width = query.shape
    span_count = seq_len // SPAN

    def to_spans(array):
        return array.reshape(number_of_heads, span_count, SPAN, array.shape[-1]).transpose(1, 0, 2, 3)
    lower_mask = jnp.tril(jnp.ones((SPAN, SPAN), bool))

    def advance(carried, inputs):
        query_span, inflow_span, decay_span, value_span = inputs
        running = jnp.cumsum(decay_span, axis=1)
        lifted_query = query_span * jnp.exp(running)
        lowered_inflow = inflow_span * jnp.exp(-running)
        scores = jnp.einsum('htd,hsd->hts', lifted_query, lowered_inflow, precision=highest)
        scores = jnp.where(lower_mask[None, :, :], scores, 0.0)
        output = jnp.einsum('hts,hsv->htv', scores, value_span, precision=highest)
        output = output + jnp.einsum('htd,hdv->htv', lifted_query, carried, precision=highest)
        closing = running[:, -1:, :]
        updated = jnp.exp(closing[:, 0, :])[:, :, None] * carried + jnp.einsum('hsd,hsv->hdv', inflow_span * jnp.exp(closing - running), value_span, precision=highest)
        return (updated, output)
    start_state = jnp.zeros((number_of_heads, key_width, values.shape[-1]), jnp.float32)
    final_state, outputs = lax.scan(advance, start_state, (to_spans(query), to_spans(inflow), to_spans(decay_logarithm), to_spans(values)))
    return (final_state, outputs.transpose(1, 0, 2, 3).reshape(number_of_heads, seq_len, values.shape[-1]))

def split_sum(left, right, groups):
    group_width = left.shape[1] // groups
    total = jnp.zeros((left.shape[0], right.shape[1]), jnp.float32)
    for portion in range(groups):
        piece = jnp.dot(left[:, portion * group_width:(portion + 1) * group_width], right[portion * group_width:(portion + 1) * group_width], preferred_element_type=jnp.float32)
        rounded = lax.optimization_barrier(piece.astype(jnp.bfloat16))
        total = total + rounded.astype(jnp.float32)
    return total.astype(jnp.bfloat16)

def reference(recurrence_query, forget_preactivation, recurrence_value, output_gate_preactivation, forget_margin, surge_log_decay, head_norm_gain, recurrence_output_matrix, second_micro_input, expert_norm_gain, routes, router_chosen_logits, expert_gate_matrix, expert_up_matrix, expert_down_matrix):
    seq_len = recurrence_query.shape[0]

    def heads_leading(array):
        return array.astype(jnp.float32).reshape(seq_len, HEADS, -1).transpose(1, 0, 2)
    closed_flag = jax.nn.sigmoid(-forget_preactivation.astype(jnp.float32)) * forget_margin
    decay_logarithm = heads_leading(jnp.log1p(-closed_flag)) + surge_log_decay[:, :, None]
    query = heads_leading(recurrence_query)
    _, output = span_recurrence(query, heads_leading(closed_flag), decay_logarithm, heads_leading(recurrence_value))
    output = output * lax.rsqrt(lax.optimization_barrier(jnp.mean(output * output, axis=-1, keepdims=True)) + epsilon)
    output = output.transpose(1, 0, 2).reshape(seq_len, -1)
    hidden_a = (output * head_norm_gain * jax.nn.silu(output_gate_preactivation.astype(jnp.float32))).astype(jnp.bfloat16)
    mixed = split_sum(hidden_a, recurrence_output_matrix, N_TP)
    moe_rows = second_micro_input.astype(jnp.float32)
    normed = (moe_rows * lax.rsqrt(lax.optimization_barrier(jnp.mean(moe_rows * moe_rows, axis=-1, keepdims=True)) + epsilon) * expert_norm_gain).astype(jnp.bfloat16)
    flat_routes = routes.reshape(-1)
    copies = flat_routes.shape[0]
    max_rows = N_EP * N_TP * CAP

    def per_expert(written, expert_id):
        picked_order = jnp.argsort((flat_routes != expert_id).astype(jnp.int32), stable=True)[:max_rows]
        picked_order = picked_order.astype(jnp.int32)
        is_live = flat_routes[picked_order] == expert_id
        picked = normed[picked_order // TOP]
        gate_proj = jnp.dot(picked, expert_gate_matrix[expert_id], preferred_element_type=jnp.float32)
        up_proj = jnp.dot(picked, expert_up_matrix[expert_id], preferred_element_type=jnp.float32)
        hidden_b = (jax.nn.silu(gate_proj) * up_proj).astype(jnp.bfloat16)
        result = split_sum(hidden_b, expert_down_matrix[expert_id], N_TP)
        kept_rows = jnp.where(is_live[:, None], result, written[picked_order])
        return (written.at[picked_order].set(kept_rows), None)
    outputs, _ = lax.scan(per_expert, jnp.zeros((copies, D), jnp.bfloat16), jnp.arange(EXPERTS, dtype=jnp.int32))
    route_weight = jax.nn.softmax(router_chosen_logits.astype(jnp.float32), axis=-1)
    moe_out = lax.optimization_barrier(jnp.sum(route_weight[:, :, None] * outputs.reshape(-1, TOP, D).astype(jnp.float32), axis=1))
    return (mixed, moe_out.astype(jnp.bfloat16))
```

```python
import functools

import jax
import jax.numpy as jnp
from jax import lax
from jax.experimental import pallas as pl
from jax.experimental.pallas import tpu as pltpu
from jax.sharding import Mesh
from jax.sharding import PartitionSpec as P

TOP = 2
SPAN = 64
CHUNKS = 8
AXES = ("ep_0", "ep_1", "ep_2", "tp")
EP = ("ep_0", "ep_1", "ep_2")
EP_TP = AXES
MESH = pl.DeviceIdType.MESH
epsilon = 1e-06
f32 = jnp.float32
bf16 = jnp.bfloat16


def dot(a, b):
    return jnp.dot(a, b, preferred_element_type=f32)


def dot_nt(a, b):
    return lax.dot_general(a, b, (((1,), (1,)), ((), ())), preferred_element_type=f32)


def dot_tn(a, b):
    return lax.dot_general(a, b, (((0,), (0,)), ((), ())), preferred_element_type=f32)


def regroup(outer, inner, slots):
    n = outer * inner * slots
    row = lax.broadcasted_iota(jnp.int32, (n, n), 0)
    col = lax.broadcasted_iota(jnp.int32, (n, n), 1)
    s_bits, i_bits = (slots - 1).bit_length(), (inner - 1).bit_length()
    o_bits = (outer - 1).bit_length()
    slot = row & (slots - 1)
    i = (row >> s_bits) & (inner - 1)
    o = row >> (s_bits + i_bits)
    source = (((i << o_bits) + o) << s_bits) + slot
    return jnp.where(col == source, 1.0, 0.0).astype(bf16)


def totals_rows(total):
    hi = total.astype(bf16).astype(f32)
    mid = (total - hi).astype(bf16).astype(f32)
    low = total - hi - mid
    rows = lax.broadcasted_iota(jnp.int32, (16, total.shape[1]), 0)
    return jnp.where(
        rows == 0, hi, jnp.where(rows == 1, mid, jnp.where(rows == 2, low, 0.0))
    ).astype(bf16)


def read_state(ref, index, rows):
    block = ref[index]
    return (
        block[:rows].astype(f32),
        jnp.sum(block[rows:].astype(f32), axis=0, keepdims=True),
    )


def chain(earlier, later):
    return (jnp.exp(later[1]) * earlier[0] + later[0], earlier[1] + later[1])


def keep_if(flag, new, old):
    return jax.tree.map(lambda a, b: jnp.where(flag, a, b), new, old)


def kernel(
    sizes,
    q_ref, f_ref, v_ref, og_ref, margin_ref, surge_ref, hgain_ref, x_ref, egain_ref, place_ref, comb_ref,
    wo_hbm, gate_hbm, up_hbm, down_hbm,
    mixed_ref, moe_ref,
    zs, zr, xs, arr, gate_v, up_v, down_v, wo_v, gacc, uacc, hb, ps, r1, r2, rx, xb, rzs, rzr,
    mp, m1, m2, s1, s2, s3, s4, s5, local_out, q_in, ha,
    w_sem, z_send, z_recv, x_send, x_recv, y_send, y_recv,
    ra_send, rb_send, r_recv, rx_send, rx_recv, rz_send, rz_recv,
    m_send, m_recv, s_send, s_recv,
):
    Z, X, C, Y, NC = sizes
    XC = X * C
    z, x, c, y = (lax.axis_index(a) for a in AXES)
    xc = x * C + c
    W = zs.shape[3]
    heads, key = surge_ref.shape[0], s4.shape[2]
    seq = q_ref.shape[0]
    quarter = s4.shape[1]
    up1, down1, across = lax.rem(y + 1, Y), lax.rem(y + Y - 1, Y), lax.rem(y + 2, Y)

    def remote(src, dst, send, recv, **at):
        return pltpu.make_async_remote_copy(
            src_ref=src,
            dst_ref=dst,
            send_sem=send,
            recv_sem=recv,
            device_id={**dict(zip(AXES, (z, x, c, y))), **at},
            device_id_type=MESH,
        )

    def await_bytes(ref, sem):
        pltpu.make_async_copy(ref, ref, sem).wait()

    def z_peers(body):
        def step(d, _):
            body(lax.rem(z + d, Z))
            return 0

        lax.fori_loop(1, Z, step, 0)

    def xc_peers(body):
        def step(d, _):
            j = lax.rem(xc + d, XC)
            body(j, j // C, lax.rem(j, C))
            return 0

        lax.fori_loop(1, XC, step, 0)

    def x_peers(body):
        def step(d, _):
            body(lax.rem(x + d, X))
            return 0

        lax.fori_loop(1, X, step, 0)

    barrier = pltpu.get_barrier_semaphore()

    def greet(**at):
        pl.semaphore_signal(
            barrier, inc=1, device_id={**dict(zip(AXES, (z, x, c, y))), **at}, device_id_type=MESH
        )

    z_peers(lambda k: greet(ep_0=k))
    xc_peers(lambda j, a, b: greet(ep_1=a, ep_2=b))
    greet(tp=up1)
    greet(tp=down1)

    weights = [
        pltpu.make_async_copy(src, dst, w_sem.at[i])
        for i, (src, dst) in enumerate(
            ((gate_hbm, gate_v), (up_hbm, up_v), (wo_hbm, wo_v), (down_hbm, down_v))
        )
    ]
    for copy in weights:
        copy.start()

    rows = x_ref[...].astype(f32)
    scale = lax.rsqrt(jnp.mean(rows * rows, axis=-1, keepdims=True) + epsilon)

    def fill(k):
        part = x_ref[:, k * W : (k + 1) * W].astype(f32)
        normed = (part * scale * egain_ref[:, k * W : (k + 1) * W]).astype(bf16)
        zs[k] = dot(place_ref[...], normed).astype(bf16).reshape(zs.shape[1:])
        zr[k, z] = zs[k, z]

    def z_go(k):
        z_peers(
            lambda d: remote(
                zs.at[k, d], zr.at[k, z], z_send.at[k], z_recv.at[k], ep_0=d
            ).start()
        )

    for k in range(NC):
        fill(k)
        if k == 0:
            pl.semaphore_wait(barrier, Z - 1 + XC - 1 + 2)
        z_go(k)

    to_xc = regroup(XC, Z, 2)
    to_z = regroup(Z, XC, 2)

    def step_a(k):
        await_bytes(zr.at[k, pl.ds(0, Z - 1)], z_recv.at[k])
        block = dot(to_xc, zr[k].reshape(-1, W)).astype(bf16)
        xs[k] = block.reshape(xs.shape[1:])
        xc_peers(
            lambda j, a, b: remote(
                xs.at[k, j], arr.at[k, 0, xc], x_send.at[k], x_recv.at[k], ep_1=a, ep_2=b
            ).start()
        )
        arr[k, 0, xc] = xs[k, xc]

    def step_b(k):
        await_bytes(arr.at[k, 0, pl.ds(0, XC - 1)], x_recv.at[k])
        remote(arr.at[k, 0], arr.at[k, 1], y_send.at[k], y_recv.at[k, 0], tp=up1).start()
        remote(arr.at[k, 0], arr.at[k, 2], y_send.at[k], y_recv.at[k, 1], tp=down1).start()

    half = XC // 2

    def step_c(k):
        await_bytes(arr.at[k, 1], y_recv.at[k, 0])
        low = pl.ds(0, half)
        remote(
            arr.at[k, 1, low], arr.at[k, 3, low], y_send.at[k], y_recv.at[k, 2], tp=up1
        ).start()
        await_bytes(arr.at[k, 2], y_recv.at[k, 1])
        high = pl.ds(half, half)
        remote(
            arr.at[k, 2, high], arr.at[k, 3, high], y_send.at[k], y_recv.at[k, 3], tp=down1
        ).start()

    def step_d(k):
        await_bytes(arr.at[k, 3, pl.ds(0, half)], y_recv.at[k, 2])
        await_bytes(arr.at[k, 3, pl.ds(half, half)], y_recv.at[k, 3])
        if k == 0:
            weights[0].wait()
            weights[1].wait()
        tokens = arr[k].reshape(-1, W)
        for acc, w in ((gacc, gate_v), (uacc, up_v)):
            part = dot(tokens, w[k * W : (k + 1) * W, :])
            if k == 0:
                acc[...] = part
            elif k < NC - 1:
                acc[...] += part
            elif acc is gacc:
                gate = acc[...] + part
            else:
                hb[...] = (jax.nn.silu(gate) * (acc[...] + part)).astype(bf16)

    def recurrence():
        shut = jax.nn.sigmoid(-f_ref[...].astype(f32)) * margin_ref[...]
        tri = jnp.where(
            lax.broadcasted_iota(jnp.int32, (seq, seq), 0)
            >= lax.broadcasted_iota(jnp.int32, (seq, seq), 1),
            1.0,
            0.0,
        )
        highest = lax.Precision.HIGHEST
        run_all = jnp.dot(tri, jnp.log1p(-shut), precision=highest, preferred_element_type=f32)
        surges = lax.dot_general(
            tri, surge_ref[...], (((1,), (1,)), ((), ())), precision=highest, preferred_element_type=f32
        )
        causal = lax.broadcasted_iota(jnp.int32, (SPAN, SPAN), 0) >= lax.broadcasted_iota(
            jnp.int32, (SPAN, SPAN), 1
        )
        for h in range(heads):
            cols = slice(h * key, (h + 1) * key)
            run = run_all[:, cols] + surges[:, h : h + 1]
            query = q_ref[:, cols].astype(f32)
            inflow = shut[:, cols]
            value = v_ref[:, cols]
            q_in[h] = (query * jnp.exp(run)).astype(bf16)
            state = None
            for i in range(seq // SPAN):
                at = slice(i * SPAN, (i + 1) * SPAN)
                r, qs, ks, vs = run[at], query[at], inflow[at], value[at]
                mid = r[SPAN // 2 : SPAN // 2 + 1]
                lifted = (qs * jnp.exp(r - mid)).astype(bf16)
                lowered = (ks * jnp.exp(mid - r)).astype(bf16)
                scores = jnp.where(causal, dot_nt(lifted, lowered), 0.0)
                out = dot(scores.astype(bf16), vs)
                close = r[SPAN - 1 : SPAN]
                added = dot_tn(vs, (ks * jnp.exp(close - r)).astype(bf16))
                if state is None:
                    state = added
                else:
                    before = run[i * SPAN - 1 : i * SPAN]
                    out = out + dot_nt((qs * jnp.exp(r - before)).astype(bf16), state.astype(bf16))
                    state = jnp.exp(close - before) * state + added
                local_out[at, cols] = out
            s1[c, h, pl.ds(0, key)] = state.astype(bf16)
            s1[c, h, pl.ds(key, 16)] = totals_rows(run[seq - 1 : seq])
        remote(s1.at[c], s1.at[c], s_send.at[0], s_recv.at[0], ep_2=1 - c).start()

    empty = lambda n: (jnp.zeros((n, key), f32), jnp.zeros((1, key), f32))

    def state_2():
        await_bytes(s1.at[1 - c], s_recv.at[0])
        both = chain(read_state(s1, (0, c), key), read_state(s1, (1, c), key))
        s2[x, pl.ds(0, key)] = both[0].astype(bf16)
        s2[x, pl.ds(key, 16)] = totals_rows(both[1])
        x_peers(
            lambda a: remote(s2.at[x], s2.at[x], s_send.at[1], s_recv.at[1], ep_1=a).start()
        )

    def x_prefix():
        prefix = empty(key)
        total = empty(key)
        for i in range(X):
            total = chain(total, read_state(s2, (i,), key))
            if i < X - 1:
                prefix = keep_if(i + 1 == x, total, prefix)
        return prefix, total

    def state_3():
        await_bytes(s2.at[pl.ds(0, X - 1)], s_recv.at[1])
        _, total = x_prefix()
        mine = total[0][:quarter]
        for i in range(1, X):
            mine = jnp.where(x == i, total[0][i * quarter : (i + 1) * quarter], mine)
        s3[z, pl.ds(0, quarter)] = mine.astype(bf16)
        s3[z, pl.ds(quarter, 16)] = totals_rows(total[1])
        z_peers(
            lambda k: remote(s3.at[z], s3.at[z], s_send.at[2], s_recv.at[2], ep_0=k).start()
        )

    def state_4():
        await_bytes(s3.at[pl.ds(0, Z - 1)], s_recv.at[2])
        prefix = empty(quarter)
        total = empty(quarter)
        for i in range(Z - 1):
            total = chain(total, read_state(s3, (i,), quarter))
            prefix = keep_if(i + 1 == z, total, prefix)
        s4[x] = prefix[0].astype(bf16)
        x_peers(
            lambda a: remote(s4.at[x], s4.at[x], s_send.at[3], s_recv.at[3], ep_1=a).start()
        )

    def state_5():
        await_bytes(s4.at[pl.ds(0, X - 1)], s_recv.at[3])
        before = s4[...].astype(f32).reshape(key, key)
        prefix, _ = x_prefix()
        s5[c] = (jnp.exp(prefix[1]) * before + prefix[0]).astype(bf16)
        remote(s5.at[c], s5.at[c], s_send.at[4], s_recv.at[4], ep_2=1 - c).start()

    def mix():
        await_bytes(s5.at[1 - c], s_recv.at[4])
        for h in range(heads):
            cols = slice(h * key, (h + 1) * key)
            chip = s5[h].astype(f32)
            first = read_state(s1, (0, h), key)
            entering = jnp.where(c == 0, chip, jnp.exp(first[1]) * chip + first[0])
            out = local_out[:, cols] + dot_nt(q_in[h], entering.astype(bf16))
            out = out * lax.rsqrt(jnp.mean(out * out, axis=-1, keepdims=True) + epsilon)
            gate = og_ref[:, cols].astype(f32)
            ha[:, cols] = (out * hgain_ref[:, cols] * jax.nn.silu(gate)).astype(bf16)
        weights[2].wait()
        for k in range(NC):
            at = slice(k * W, (k + 1) * W)
            mp[:, :, :, at] = dot(ha[...], wo_v[:, at]).astype(bf16).reshape(mp.shape[:3] + (W,))

    def mix_a():
        remote(mp.at[across, 0], m1.at[0], m_send.at[0], m_recv.at[0], tp=up1).start()
        remote(mp.at[across, 1], m1.at[1], m_send.at[0], m_recv.at[1], tp=down1).start()

    def mix_b():
        for i, to in ((0, up1), (1, down1)):
            await_bytes(m1.at[i], m_recv.at[i])
            mp[to, i] = (mp[to, i].astype(f32) + m1[i].astype(f32)).astype(bf16)
            remote(mp.at[to], m2.at[i], m_send.at[1], m_recv.at[2 + i], tp=to).start()

    def mix_c():
        await_bytes(m2.at[0], m_recv.at[2])
        await_bytes(m2.at[1], m_recv.at[3])
        total = mp[y].astype(f32) + m2[0].astype(f32) + m2[1].astype(f32)
        mixed_ref[...] = total.astype(bf16).reshape(mixed_ref.shape)

    def step_e(k):
        if k == 0:
            weights[3].wait()
        part = dot(hb[...], down_v[:, k * W : (k + 1) * W])
        ps[k] = part.astype(bf16).reshape(ps.shape[1:])
        remote(ps.at[k, 3, 0], r1.at[k, 0], ra_send.at[k], r_recv.at[k, 0], tp=up1).start()
        remote(ps.at[k, 3, 1], r1.at[k, 1], ra_send.at[k], r_recv.at[k, 1], tp=down1).start()

    def step_f(k):
        for i, rel, to in ((0, 2, up1), (1, 1, down1)):
            await_bytes(r1.at[k, i], r_recv.at[k, i])
            ps[k, rel, i] = (ps[k, rel, i].astype(f32) + r1[k, i].astype(f32)).astype(bf16)
            remote(ps.at[k, rel], r2.at[k, i], rb_send.at[k], r_recv.at[k, 2 + i], tp=to).start()

    def step_g(k):
        await_bytes(r2.at[k, 0], r_recv.at[k, 2])
        await_bytes(r2.at[k, 1], r_recv.at[k, 3])
        total = ps[k, 0].astype(f32) + r2[k, 0].astype(f32) + r2[k, 1].astype(f32)
        rx[k] = total.astype(bf16).reshape(rx.shape[1:])
        xc_peers(
            lambda j, a, b: remote(
                rx.at[k, j], xb.at[k, xc], rx_send.at[k], rx_recv.at[k], ep_1=a, ep_2=b
            ).start()
        )
        xb[k, xc] = rx[k, xc]

    def step_h(k):
        await_bytes(xb.at[k, pl.ds(0, XC - 1)], rx_recv.at[k])
        block = dot(to_z, xb[k].reshape(-1, W)).astype(bf16)
        rzs[k] = block.reshape(rzs.shape[1:])
        z_peers(
            lambda d: remote(
                rzs.at[k, d], rzr.at[k, z], rz_send.at[k], rz_recv.at[k], ep_0=d
            ).start()
        )
        rzr[k, z] = rzs[k, z]

    comb_hi = comb_ref[...].astype(bf16)
    comb_lo = (comb_ref[...] - comb_hi.astype(f32)).astype(bf16)

    def step_i(k):
        await_bytes(rzr.at[k, pl.ds(0, Z - 1)], rz_recv.at[k])
        results = rzr[k].reshape(-1, W)
        moe_ref[:, k * W : (k + 1) * W] = (dot(comb_hi, results) + dot(comb_lo, results)).astype(bf16)

    recurrence()
    side = {0: state_2, 1: state_3, 3: state_4, 4: state_5, 5: mix}
    last = NC + 3
    for t in range(last):
        if t < NC:
            step_a(t)
        if 0 <= t - 1 < NC:
            step_b(t - 1)
        if t - 1 == NC - 1:
            mix_a()
        if 0 <= t - 2 < NC:
            step_c(t - 2)
        if t - 2 == NC - 1:
            mix_b()
        if 0 <= t - 3 < NC:
            step_d(t - 3)
        if t in side:
            side[t]()
    for t in range(NC + 4):
        if t < NC:
            step_e(t)
        if 0 <= t - 1 < NC:
            step_f(t - 1)
        if 0 <= t - 2 < NC:
            step_g(t - 2)
        if 0 <= t - 3 < NC:
            step_h(t - 3)
        if 0 <= t - 4 < NC:
            step_i(t - 4)
        if t == 2:
            mix_c()

    for k in range(NC):
        await_bytes(zs.at[k, pl.ds(0, Z - 1)], z_send.at[k])
        await_bytes(xs.at[k, pl.ds(0, XC - 1)], x_send.at[k])
        await_bytes(arr.at[k, pl.ds(0, 3)], y_send.at[k])
        await_bytes(ps.at[k, 3], ra_send.at[k])
        await_bytes(ps.at[k, pl.ds(1, 2)], rb_send.at[k])
        await_bytes(rx.at[k, pl.ds(0, XC - 1)], rx_send.at[k])
        await_bytes(rzs.at[k, pl.ds(0, Z - 1)], rz_send.at[k])
    await_bytes(mp.at[0], m_send.at[0])
    await_bytes(mp.at[pl.ds(0, 2)], m_send.at[1])
    await_bytes(s1.at[0], s_send.at[0])
    await_bytes(s2.at[pl.ds(0, X - 1)], s_send.at[1])
    await_bytes(s3.at[pl.ds(0, Z - 1)], s_send.at[2])
    await_bytes(s4.at[pl.ds(0, X - 1)], s_send.at[3])
    await_bytes(s5.at[0], s_send.at[4])


def slot_tables(block_routes, logits, experts):
    chosen = block_routes.reshape(-1)
    table = (chosen[:, None] == jnp.arange(experts, dtype=jnp.int32)[None, :]).astype(jnp.int32)
    before = jnp.cumsum(table, axis=0) - table
    slot = chosen * 2 + jnp.sum(before * table, axis=1)
    taken = slot[:, None] == jnp.arange(2 * experts, dtype=jnp.int32)[None, :]
    weight = jax.nn.softmax(logits, axis=-1).reshape(-1)
    tokens = block_routes.shape[0]
    place = jnp.any(taken.reshape(tokens, TOP, -1), axis=1).astype(bf16).T
    comb = jnp.sum(jnp.where(taken, weight[:, None], 0.0).reshape(tokens, TOP, -1), axis=1)
    return place, comb


def per_device(
    sizes,
    recurrence_query,
    forget_preactivation,
    recurrence_value,
    output_gate_preactivation,
    forget_margin,
    surge_log_decay,
    head_norm_gain,
    recurrence_output_matrix,
    second_micro_input,
    expert_norm_gain,
    routes,
    router_chosen_logits,
    expert_gate_matrix,
    expert_up_matrix,
    expert_down_matrix,
):
    Z, X, C, Y, NC = sizes
    XC = X * C
    experts = Z * XC
    tokens, D = second_micro_input.shape
    seq, width = recurrence_query.shape
    heads = surge_log_decay.shape[0]
    key = width // heads
    F = expert_gate_matrix.shape[2]
    W = D // NC
    own_routes = lax.dynamic_slice_in_dim(routes, lax.axis_index("tp") * tokens, tokens, 0)
    place, comb = slot_tables(own_routes, router_chosen_logits, experts)
    slots = 2 * experts
    V = pltpu.VMEM
    DMA = pltpu.SemaphoreType.DMA
    scratch = [
        V((NC, Z, 2 * XC, W), bf16),
        V((NC, Z, 2 * XC, W), bf16),
        V((NC, XC, 2 * Z, W), bf16),
        V((NC, Y, XC, 2 * Z, W), bf16),
        V((D, F), bf16),
        V((D, F), bf16),
        V((F, D), bf16),
        V((width, D), bf16),
        V((Y * slots, F), f32),
        V((Y * slots, F), f32),
        V((Y * slots, F), bf16),
        V((NC, Y, 2, slots // 2, W), bf16),
        V((NC, 2, slots // 2, W), bf16),
        V((NC, 2, 2, slots // 2, W), bf16),
        V((NC, XC, 2 * Z, W), bf16),
        V((NC, XC, 2 * Z, W), bf16),
        V((NC, Z, 2 * XC, W), bf16),
        V((NC, Z, 2 * XC, W), bf16),
        V((Y, 2, seq // Y // 2, D), bf16),
        V((2, seq // Y // 2, D), bf16),
        V((2, 2, seq // Y // 2, D), bf16),
        V((C, heads, key + 16, key), bf16),
        V((X, key + 16, key), bf16),
        V((Z, key // X + 16, key), bf16),
        V((X, key // X, key), bf16),
        V((C, key, key), bf16),
        V((seq, width), f32),
        V((heads, seq, key), bf16),
        V((seq, width), bf16),
        DMA((4,)),
        DMA((NC,)),
        DMA((NC,)),
        DMA((NC,)),
        DMA((NC,)),
        DMA((NC,)),
        DMA((NC, 4)),
        DMA((NC,)),
        DMA((NC,)),
        DMA((NC, 4)),
        DMA((NC,)),
        DMA((NC,)),
        DMA((NC,)),
        DMA((NC,)),
        DMA((2,)),
        DMA((4,)),
        DMA((5,)),
        DMA((5,)),
    ]
    vmem = pl.BlockSpec(memory_space=pltpu.VMEM)
    hbm = pl.BlockSpec(memory_space=pl.ANY)
    out = jax.ShapeDtypeStruct((tokens, D), bf16)
    return pl.pallas_call(
        functools.partial(kernel, sizes),
        out_shape=(jax.ShapeDtypeStruct((seq // Y, D), bf16), out),
        in_specs=[vmem] * 11 + [hbm] * 4,
        out_specs=(vmem, vmem),
        scratch_shapes=scratch,
        compiler_params=pltpu.CompilerParams(
            collective_id=0, has_side_effects=True, vmem_limit_bytes=63 * 1024 * 1024
        ),
    )(
        recurrence_query,
        forget_preactivation,
        recurrence_value,
        output_gate_preactivation,
        forget_margin.reshape(1, -1),
        surge_log_decay,
        head_norm_gain.reshape(1, -1),
        second_micro_input,
        expert_norm_gain.reshape(1, -1),
        place,
        comb,
        recurrence_output_matrix,
        expert_gate_matrix[0],
        expert_up_matrix[0],
        expert_down_matrix[0],
    )


def build(finer, chunks):
    sizes = tuple(finer.shape[a] for a in AXES) + (chunks,)
    in_specs = (
        P(EP, "tp"),
        P(EP, "tp"),
        P(EP, "tp"),
        P(EP, "tp"),
        P("tp"),
        P("tp", EP),
        P("tp"),
        P("tp", None),
        P(EP_TP, None),
        P(),
        P(EP, None),
        P(EP_TP, None),
        P(EP, None, "tp"),
        P(EP, None, "tp"),
        P(EP, "tp", None),
    )
    out_specs = (P(EP_TP, None), P(EP_TP, None))
    return jax.shard_map(
        functools.partial(per_device, sizes),
        mesh=finer,
        in_specs=in_specs,
        out_specs=out_specs,
        check_vma=False,
    )


def solution(mesh):
    return build(Mesh(mesh.devices.reshape(8, 4, 2, mesh.shape["tp"]), AXES), CHUNKS)
```

```python
import functools

import jax
import jax.numpy as jnp
from jax import lax
from jax.experimental import pallas as pl
from jax.experimental.pallas import tpu as pltpu
from jax.sharding import Mesh
from jax.sharding import PartitionSpec as P

TOP = 2
SPAN = 64
CHUNKS = 8
AXES = ("ep_0", "ep_1", "ep_2", "tp")
EP = ("ep_0", "ep_1", "ep_2")
EP_TP = AXES
MESH = pl.DeviceIdType.MESH
epsilon = 1e-06
f32 = jnp.float32
bf16 = jnp.bfloat16


def dot(a, b):
    return jnp.dot(a, b, preferred_element_type=f32)


def dot_nt(a, b):
    return lax.dot_general(a, b, (((1,), (1,)), ((), ())), preferred_element_type=f32)


def dot_tn(a, b):
    return lax.dot_general(a, b, (((0,), (0,)), ((), ())), preferred_element_type=f32)


def regroup(outer, inner, slots):
    n = outer * inner * slots
    row = lax.broadcasted_iota(jnp.int32, (n, n), 0)
    col = lax.broadcasted_iota(jnp.int32, (n, n), 1)
    s_bits, i_bits = (slots - 1).bit_length(), (inner - 1).bit_length()
    o_bits = (outer - 1).bit_length()
    slot = row & (slots - 1)
    i = (row >> s_bits) & (inner - 1)
    o = row >> (s_bits + i_bits)
    source = (((i << o_bits) + o) << s_bits) + slot
    return jnp.where(col == source, 1.0, 0.0).astype(bf16)


def totals_rows(total):
    hi = total.astype(bf16).astype(f32)
    mid = (total - hi).astype(bf16).astype(f32)
    low = total - hi - mid
    rows = lax.broadcasted_iota(jnp.int32, (16, total.shape[1]), 0)
    return jnp.where(
        rows == 0, hi, jnp.where(rows == 1, mid, jnp.where(rows == 2, low, 0.0))
    ).astype(bf16)


def read_state(ref, index, rows):
    block = ref[index]
    return (
        block[:rows].astype(f32),
        jnp.sum(block[rows:].astype(f32), axis=0, keepdims=True),
    )


def chain(earlier, later):
    return (jnp.exp(later[1]) * earlier[0] + later[0], earlier[1] + later[1])


def keep_if(flag, new, old):
    return jax.tree.map(lambda a, b: jnp.where(flag, a, b), new, old)


def kernel(
    sizes,
    q_ref, f_ref, v_ref, og_ref, margin_ref, surge_ref, hgain_ref, x_ref, egain_ref, routes_ref, logits_ref,
    wo_hbm, gate_hbm, up_hbm, down_hbm,
    mixed_ref, moe_ref,
    zs, zr, xs, arr, gate_v, up_v, down_v, wo_v, gacc, uacc, hb, ps, r1, r2, rx, xb, rzs, rzr,
    mp, m1, m2, s1, s2, s3, s4, s5, local_out, q_in, ha,
    w_sem, z_send, z_recv, x_send, x_recv, y_send, y_recv,
    ra_send, rb_send, r_recv, rx_send, rx_recv, rz_send, rz_recv,
    m_send, m_recv, s_send, s_recv,
):
    Z, X, C, Y, NC = sizes
    XC = X * C
    z, x, c, y = (lax.axis_index(a) for a in AXES)
    xc = x * C + c
    W = zs.shape[3]
    heads, key = surge_ref.shape[0], s4.shape[2]
    seq = q_ref.shape[0]
    quarter = s4.shape[1]
    up1, down1, across = lax.rem(y + 1, Y), lax.rem(y + Y - 1, Y), lax.rem(y + 2, Y)

    z_at = [lax.rem(z + d, Z) for d in range(Z)]
    xc_at = [lax.rem(xc + d, XC) for d in range(XC)]
    xc_at = [(j, j // C, lax.rem(j, C)) for j in xc_at]

    def remote(src, dst, send, recv, **at):
        return pltpu.make_async_remote_copy(
            src_ref=src,
            dst_ref=dst,
            send_sem=send,
            recv_sem=recv,
            device_id={**dict(zip(AXES, (z, x, c, y))), **at},
            device_id_type=MESH,
        )

    def await_bytes(ref, sem):
        pltpu.make_async_copy(ref, ref, sem).wait()

    def z_peers(body):
        for d in range(1, Z):
            body(z_at[d])

    def xc_peers(body):
        for d in range(1, XC):
            body(*xc_at[d])

    def x_peers(body):
        for d in range(1, X):
            body(lax.rem(x + d, X))

    barrier = pltpu.get_barrier_semaphore()

    def greet(**at):
        pl.semaphore_signal(
            barrier, inc=1, device_id={**dict(zip(AXES, (z, x, c, y))), **at}, device_id_type=MESH
        )

    z_peers(lambda k: greet(ep_0=k))
    xc_peers(lambda j, a, b: greet(ep_1=a, ep_2=b))
    greet(tp=up1)
    greet(tp=down1)

    weights = [
        pltpu.make_async_copy(src, dst, w_sem.at[i])
        for i, (src, dst) in enumerate(
            ((gate_hbm, gate_v), (up_hbm, up_v), (wo_hbm, wo_v), (down_hbm, down_v))
        )
    ]
    for copy in weights:
        copy.start()

    tokens = x_ref.shape[0]
    chosen = routes_ref[:, :tokens]
    for i in range(1, Y):
        chosen = jnp.where(y == i, routes_ref[:, i * tokens : (i + 1) * tokens], chosen)
    place, comb = slot_tables(chosen, logits_ref[...], Z * XC)
    rows = x_ref[...].astype(f32)
    scale = lax.rsqrt(jnp.mean(rows * rows, axis=-1, keepdims=True) + epsilon)

    def fill(k):
        part = x_ref[:, k * W : (k + 1) * W].astype(f32)
        normed = (part * scale * egain_ref[:, k * W : (k + 1) * W]).astype(bf16)
        zs[k] = dot(place, normed).astype(bf16).reshape(zs.shape[1:])
        zr[k, z] = zs[k, z]

    def z_go(k):
        z_peers(
            lambda d: remote(
                zs.at[k, d], zr.at[k, z], z_send.at[k], z_recv.at[k], ep_0=d
            ).start()
        )

    for k in range(NC):
        fill(k)
        if k == 0:
            pl.semaphore_wait(barrier, Z - 1 + XC - 1 + 2)
        z_go(k)

    to_xc = regroup(XC, Z, 2)
    to_z = regroup(Z, XC, 2)

    def step_a(k):
        await_bytes(zr.at[k, pl.ds(0, Z - 1)], z_recv.at[k])
        block = dot(to_xc, zr[k].reshape(-1, W)).astype(bf16)
        xs[k] = block.reshape(xs.shape[1:])
        xc_peers(
            lambda j, a, b: remote(
                xs.at[k, j], arr.at[k, 0, xc], x_send.at[k], x_recv.at[k], ep_1=a, ep_2=b
            ).start()
        )
        arr[k, 0, xc] = xs[k, xc]

    def step_b(k):
        await_bytes(arr.at[k, 0, pl.ds(0, XC - 1)], x_recv.at[k])
        remote(arr.at[k, 0], arr.at[k, 1], y_send.at[k], y_recv.at[k, 0], tp=up1).start()
        remote(arr.at[k, 0], arr.at[k, 2], y_send.at[k], y_recv.at[k, 1], tp=down1).start()

    half = XC // 2

    def step_c(k):
        await_bytes(arr.at[k, 1], y_recv.at[k, 0])
        low = pl.ds(0, half)
        remote(
            arr.at[k, 1, low], arr.at[k, 3, low], y_send.at[k], y_recv.at[k, 2], tp=up1
        ).start()
        await_bytes(arr.at[k, 2], y_recv.at[k, 1])
        high = pl.ds(half, half)
        remote(
            arr.at[k, 2, high], arr.at[k, 3, high], y_send.at[k], y_recv.at[k, 3], tp=down1
        ).start()

    def step_d(k):
        await_bytes(arr.at[k, 3, pl.ds(0, half)], y_recv.at[k, 2])
        await_bytes(arr.at[k, 3, pl.ds(half, half)], y_recv.at[k, 3])
        if k == 0:
            weights[0].wait()
            weights[1].wait()
        tokens = arr[k].reshape(-1, W)
        for acc, w in ((gacc, gate_v), (uacc, up_v)):
            part = dot_nt(tokens, w[:, k * W : (k + 1) * W])
            if k == 0:
                acc[...] = part
            elif k < NC - 1:
                acc[...] += part
            elif acc is gacc:
                gate = acc[...] + part
            else:
                hb[...] = (jax.nn.silu(gate) * (acc[...] + part)).astype(bf16)

    def recurrence():
        shut = jax.nn.sigmoid(-f_ref[...].astype(f32)) * margin_ref[...]
        tri = jnp.where(
            lax.broadcasted_iota(jnp.int32, (seq, seq), 0)
            >= lax.broadcasted_iota(jnp.int32, (seq, seq), 1),
            1.0,
            0.0,
        )
        highest = lax.Precision.HIGHEST
        run_all = jnp.dot(tri, jnp.log1p(-shut), precision=highest, preferred_element_type=f32)
        surges = lax.dot_general(
            tri, surge_ref[...], (((1,), (1,)), ((), ())), precision=highest, preferred_element_type=f32
        )
        causal = lax.broadcasted_iota(jnp.int32, (SPAN, SPAN), 0) >= lax.broadcasted_iota(
            jnp.int32, (SPAN, SPAN), 1
        )
        for h in range(heads):
            cols = slice(h * key, (h + 1) * key)
            run = run_all[:, cols] + surges[:, h : h + 1]
            query = q_ref[:, cols].astype(f32)
            inflow = shut[:, cols]
            value = v_ref[:, cols]
            q_in[h] = (query * jnp.exp(run)).astype(bf16)
            state = None
            for i in range(seq // SPAN):
                at = slice(i * SPAN, (i + 1) * SPAN)
                r, qs, ks, vs = run[at], query[at], inflow[at], value[at]
                mid = r[SPAN // 2 : SPAN // 2 + 1]
                lifted = (qs * jnp.exp(r - mid)).astype(bf16)
                lowered = (ks * jnp.exp(mid - r)).astype(bf16)
                scores = jnp.where(causal, dot_nt(lifted, lowered), 0.0)
                out = dot(scores.astype(bf16), vs)
                close = r[SPAN - 1 : SPAN]
                added = dot_tn(vs, (ks * jnp.exp(close - r)).astype(bf16))
                if state is None:
                    state = added
                else:
                    before = run[i * SPAN - 1 : i * SPAN]
                    out = out + dot_nt((qs * jnp.exp(r - before)).astype(bf16), state.astype(bf16))
                    state = jnp.exp(close - before) * state + added
                local_out[at, cols] = out
            s1[c, h, pl.ds(0, key)] = state.astype(bf16)
            s1[c, h, pl.ds(key, 16)] = totals_rows(run[seq - 1 : seq])
        remote(s1.at[c], s1.at[c], s_send.at[0], s_recv.at[0], ep_2=1 - c).start()

    empty = lambda n: (jnp.zeros((n, key), f32), jnp.zeros((1, key), f32))

    def state_2():
        await_bytes(s1.at[1 - c], s_recv.at[0])
        both = chain(read_state(s1, (0, c), key), read_state(s1, (1, c), key))
        s2[x, pl.ds(0, key)] = both[0].astype(bf16)
        s2[x, pl.ds(key, 16)] = totals_rows(both[1])
        x_peers(
            lambda a: remote(s2.at[x], s2.at[x], s_send.at[1], s_recv.at[1], ep_1=a).start()
        )

    def x_prefix():
        prefix = empty(key)
        total = empty(key)
        for i in range(X):
            total = chain(total, read_state(s2, (i,), key))
            if i < X - 1:
                prefix = keep_if(i + 1 == x, total, prefix)
        return prefix, total

    def state_3():
        await_bytes(s2.at[pl.ds(0, X - 1)], s_recv.at[1])
        _, total = x_prefix()
        mine = total[0][:quarter]
        for i in range(1, X):
            mine = jnp.where(x == i, total[0][i * quarter : (i + 1) * quarter], mine)
        s3[z, pl.ds(0, quarter)] = mine.astype(bf16)
        s3[z, pl.ds(quarter, 16)] = totals_rows(total[1])
        z_peers(
            lambda k: remote(s3.at[z], s3.at[z], s_send.at[2], s_recv.at[2], ep_0=k).start()
        )

    def state_4():
        await_bytes(s3.at[pl.ds(0, Z - 1)], s_recv.at[2])
        prefix = empty(quarter)
        total = empty(quarter)
        for i in range(Z - 1):
            total = chain(total, read_state(s3, (i,), quarter))
            prefix = keep_if(i + 1 == z, total, prefix)
        s4[x] = prefix[0].astype(bf16)
        x_peers(
            lambda a: remote(s4.at[x], s4.at[x], s_send.at[3], s_recv.at[3], ep_1=a).start()
        )

    def state_5():
        await_bytes(s4.at[pl.ds(0, X - 1)], s_recv.at[3])
        before = s4[...].astype(f32).reshape(key, key)
        prefix, _ = x_prefix()
        s5[c] = (jnp.exp(prefix[1]) * before + prefix[0]).astype(bf16)
        remote(s5.at[c], s5.at[c], s_send.at[4], s_recv.at[4], ep_2=1 - c).start()

    def mix():
        await_bytes(s5.at[1 - c], s_recv.at[4])
        for h in range(heads):
            cols = slice(h * key, (h + 1) * key)
            chip = s5[h].astype(f32)
            first = read_state(s1, (0, h), key)
            entering = jnp.where(c == 0, chip, jnp.exp(first[1]) * chip + first[0])
            out = local_out[:, cols] + dot_nt(q_in[h], entering.astype(bf16))
            out = out * lax.rsqrt(jnp.mean(out * out, axis=-1, keepdims=True) + epsilon)
            gate = og_ref[:, cols].astype(f32)
            ha[:, cols] = (out * hgain_ref[:, cols] * jax.nn.silu(gate)).astype(bf16)
        weights[2].wait()
        for k in range(NC):
            at = slice(k * W, (k + 1) * W)
            mp[:, :, :, at] = dot(ha[...], wo_v[:, at]).astype(bf16).reshape(mp.shape[:3] + (W,))

    def mix_a():
        remote(mp.at[across, 0], m1.at[0], m_send.at[0], m_recv.at[0], tp=up1).start()
        remote(mp.at[across, 1], m1.at[1], m_send.at[0], m_recv.at[1], tp=down1).start()

    def mix_b():
        for i, to in ((0, up1), (1, down1)):
            await_bytes(m1.at[i], m_recv.at[i])
            mp[to, i] = (mp[to, i].astype(f32) + m1[i].astype(f32)).astype(bf16)
            remote(mp.at[to], m2.at[i], m_send.at[1], m_recv.at[2 + i], tp=to).start()

    def mix_c():
        await_bytes(m2.at[0], m_recv.at[2])
        await_bytes(m2.at[1], m_recv.at[3])
        total = mp[y].astype(f32) + m2[0].astype(f32) + m2[1].astype(f32)
        mixed_ref[...] = total.astype(bf16).reshape(mixed_ref.shape)

    def step_e(k):
        if k == 0:
            weights[3].wait()
        part = dot(hb[...], down_v[:, k * W : (k + 1) * W])
        ps[k] = part.astype(bf16).reshape(ps.shape[1:])
        remote(ps.at[k, 3, 0], r1.at[k, 0], ra_send.at[k], r_recv.at[k, 0], tp=up1).start()
        remote(ps.at[k, 3, 1], r1.at[k, 1], ra_send.at[k], r_recv.at[k, 1], tp=down1).start()

    def step_f(k):
        for i, rel, to in ((0, 2, up1), (1, 1, down1)):
            await_bytes(r1.at[k, i], r_recv.at[k, i])
            ps[k, rel, i] = (ps[k, rel, i].astype(f32) + r1[k, i].astype(f32)).astype(bf16)
            remote(ps.at[k, rel], r2.at[k, i], rb_send.at[k], r_recv.at[k, 2 + i], tp=to).start()

    def step_g(k):
        await_bytes(r2.at[k, 0], r_recv.at[k, 2])
        await_bytes(r2.at[k, 1], r_recv.at[k, 3])
        total = ps[k, 0].astype(f32) + r2[k, 0].astype(f32) + r2[k, 1].astype(f32)
        rx[k] = total.astype(bf16).reshape(rx.shape[1:])
        xc_peers(
            lambda j, a, b: remote(
                rx.at[k, j], xb.at[k, xc], rx_send.at[k], rx_recv.at[k], ep_1=a, ep_2=b
            ).start()
        )
        xb[k, xc] = rx[k, xc]

    def step_h(k):
        await_bytes(xb.at[k, pl.ds(0, XC - 1)], rx_recv.at[k])
        block = dot(to_z, xb[k].reshape(-1, W)).astype(bf16)
        rzs[k] = block.reshape(rzs.shape[1:])
        z_peers(
            lambda d: remote(
                rzs.at[k, d], rzr.at[k, z], rz_send.at[k], rz_recv.at[k], ep_0=d
            ).start()
        )
        rzr[k, z] = rzs[k, z]

    comb = comb.T
    comb_hi = comb.astype(bf16)
    comb_lo = (comb - comb_hi.astype(f32)).astype(bf16)

    def step_i(k):
        await_bytes(rzr.at[k, pl.ds(0, Z - 1)], rz_recv.at[k])
        results = rzr[k].reshape(-1, W)
        moe_ref[:, k * W : (k + 1) * W] = (dot(comb_hi, results) + dot(comb_lo, results)).astype(bf16)

    recurrence()
    for t in range(NC + 3):
        if t < NC:
            step_a(t)
        if t == NC + 1:
            mix()
        if 0 <= t - 1 < NC:
            step_b(t - 1)
        if 0 <= t - 2 < NC:
            step_c(t - 2)
        if t == NC + 1:
            mix_a()
        if t == 0:
            state_2()
        if t == 1:
            state_3()
        if t == NC:
            state_4()
        if 0 <= t - 3 < NC:
            step_d(t - 3)
        if t == NC:
            state_5()
    for t in range(NC + 4):
        if t < NC:
            step_e(t)
        if 0 <= t - 1 < NC:
            step_f(t - 1)
        if t == NC:
            mix_b()
        if 0 <= t - 2 < NC:
            step_g(t - 2)
        if 0 <= t - 3 < NC:
            step_h(t - 3)
        if t == NC + 2:
            mix_c()
        if 0 <= t - 4 < NC:
            step_i(t - 4)

    for k in range(NC):
        await_bytes(zs.at[k, pl.ds(0, Z - 1)], z_send.at[k])
        await_bytes(xs.at[k, pl.ds(0, XC - 1)], x_send.at[k])
        await_bytes(arr.at[k, pl.ds(0, 3)], y_send.at[k])
        await_bytes(ps.at[k, 3], ra_send.at[k])
        await_bytes(ps.at[k, pl.ds(1, 2)], rb_send.at[k])
        await_bytes(rx.at[k, pl.ds(0, XC - 1)], rx_send.at[k])
        await_bytes(rzs.at[k, pl.ds(0, Z - 1)], rz_send.at[k])
    await_bytes(mp.at[0], m_send.at[0])
    await_bytes(mp.at[pl.ds(0, 2)], m_send.at[1])
    await_bytes(s1.at[0], s_send.at[0])
    await_bytes(s2.at[pl.ds(0, X - 1)], s_send.at[1])
    await_bytes(s3.at[pl.ds(0, Z - 1)], s_send.at[2])
    await_bytes(s4.at[pl.ds(0, X - 1)], s_send.at[3])
    await_bytes(s5.at[0], s_send.at[4])


def slot_tables(chosen, logits, experts):
    tokens = chosen.shape[1]
    top = jnp.max(logits, axis=0, keepdims=True)
    raised = jnp.exp(logits - top)
    weight = raised / jnp.sum(raised, axis=0, keepdims=True)
    expert = lax.broadcasted_iota(jnp.int32, (experts, tokens), 0)
    named = [jnp.where(expert == chosen[j : j + 1], 1.0, 0.0) for j in range(TOP)]
    earlier = lax.broadcasted_iota(jnp.int32, (tokens, tokens), 0) < lax.broadcasted_iota(
        jnp.int32, (tokens, tokens), 1
    )
    before = dot(sum(named).astype(bf16), jnp.where(earlier, 1.0, 0.0).astype(bf16))
    row = lax.broadcasted_iota(jnp.int32, (2 * experts, tokens), 0).astype(f32)
    place = jnp.zeros((2 * experts, tokens), f32)
    comb = place
    for j in range(TOP):
        rank = jnp.sum(named[j] * before, axis=0, keepdims=True)
        here = row == 2.0 * chosen[j : j + 1].astype(f32) + rank
        place = jnp.where(here, 1.0, place)
        comb = jnp.where(here, weight[j : j + 1], comb)
    return place.astype(bf16), comb


def hand_on(mixed_in, moe_in, mixed_out, moe_out):
    mixed_out[...] = mixed_in[...]
    moe_out[...] = moe_in[...]


def per_device(
    sizes,
    recurrence_query,
    forget_preactivation,
    recurrence_value,
    output_gate_preactivation,
    forget_margin,
    surge_log_decay,
    head_norm_gain,
    recurrence_output_matrix,
    second_micro_input,
    expert_norm_gain,
    routes,
    router_chosen_logits,
    expert_gate_matrix,
    expert_up_matrix,
    expert_down_matrix,
):
    Z, X, C, Y, NC = sizes
    XC = X * C
    experts = Z * XC
    tokens, D = second_micro_input.shape
    seq, width = recurrence_query.shape
    heads = surge_log_decay.shape[0]
    key = width // heads
    F = expert_gate_matrix.shape[2]
    W = D // NC
    slots = 2 * experts
    V = pltpu.VMEM
    DMA = pltpu.SemaphoreType.DMA
    scratch = [
        V((NC, Z, 2 * XC, W), bf16),
        V((NC, Z, 2 * XC, W), bf16),
        V((NC, XC, 2 * Z, W), bf16),
        V((NC, Y, XC, 2 * Z, W), bf16),
        V((F, D), bf16),
        V((F, D), bf16),
        V((F, D), bf16),
        V((width, D), bf16),
        V((Y * slots, F), f32),
        V((Y * slots, F), f32),
        V((Y * slots, F), bf16),
        V((NC, Y, 2, slots // 2, W), bf16),
        V((NC, 2, slots // 2, W), bf16),
        V((NC, 2, 2, slots // 2, W), bf16),
        V((NC, XC, 2 * Z, W), bf16),
        V((NC, XC, 2 * Z, W), bf16),
        V((NC, Z, 2 * XC, W), bf16),
        V((NC, Z, 2 * XC, W), bf16),
        V((Y, 2, seq // Y // 2, D), bf16),
        V((2, seq // Y // 2, D), bf16),
        V((2, 2, seq // Y // 2, D), bf16),
        V((C, heads, key + 16, key), bf16),
        V((X, key + 16, key), bf16),
        V((Z, key // X + 16, key), bf16),
        V((X, key // X, key), bf16),
        V((C, key, key), bf16),
        V((seq, width), f32),
        V((heads, seq, key), bf16),
        V((seq, width), bf16),
        DMA((4,)),
        DMA((NC,)),
        DMA((NC,)),
        DMA((NC,)),
        DMA((NC,)),
        DMA((NC,)),
        DMA((NC, 4)),
        DMA((NC,)),
        DMA((NC,)),
        DMA((NC, 4)),
        DMA((NC,)),
        DMA((NC,)),
        DMA((NC,)),
        DMA((NC,)),
        DMA((2,)),
        DMA((4,)),
        DMA((5,)),
        DMA((5,)),
    ]
    vmem = pl.BlockSpec(memory_space=pltpu.VMEM)
    hbm = pl.BlockSpec(memory_space=pl.ANY)
    out = jax.ShapeDtypeStruct((tokens, D), bf16)
    results = pl.pallas_call(
        functools.partial(kernel, sizes),
        out_shape=(jax.ShapeDtypeStruct((seq // Y, D), bf16), out),
        in_specs=[vmem] * 11 + [hbm] * 4,
        out_specs=(vmem, vmem),
        scratch_shapes=scratch,
        compiler_params=pltpu.CompilerParams(
            collective_id=0, has_side_effects=True, vmem_limit_bytes=63 * 1024 * 1024
        ),
    )(
        recurrence_query,
        forget_preactivation,
        recurrence_value,
        output_gate_preactivation,
        forget_margin.reshape(1, -1),
        surge_log_decay,
        head_norm_gain.reshape(1, -1),
        second_micro_input,
        expert_norm_gain.reshape(1, -1),
        routes.T,
        router_chosen_logits.T,
        recurrence_output_matrix,
        expert_gate_matrix[0].T,
        expert_up_matrix[0].T,
        expert_down_matrix[0],
    )
    return pl.pallas_call(
        hand_on,
        out_shape=(jax.ShapeDtypeStruct((seq // Y, D), bf16), out),
        in_specs=[vmem] * 2,
        out_specs=(vmem, vmem),
    )(*results)


def build(finer, chunks):
    sizes = tuple(finer.shape[a] for a in AXES) + (chunks,)
    in_specs = (
        P(EP, "tp"),
        P(EP, "tp"),
        P(EP, "tp"),
        P(EP, "tp"),
        P("tp"),
        P("tp", EP),
        P("tp"),
        P("tp", None),
        P(EP_TP, None),
        P(),
        P(EP, None),
        P(EP_TP, None),
        P(EP, None, "tp"),
        P(EP, None, "tp"),
        P(EP, "tp", None),
    )
    out_specs = (P(EP_TP, None), P(EP_TP, None))
    return jax.shard_map(
        functools.partial(per_device, sizes),
        mesh=finer,
        in_specs=in_specs,
        out_specs=out_specs,
        check_vma=False,
    )


def solution(mesh):
    return build(Mesh(mesh.devices.reshape(8, 4, 2, mesh.shape["tp"]), AXES), CHUNKS)
```

```python
import functools

import jax
import jax.numpy as jnp
from jax import lax
from jax.experimental import pallas as pl
from jax.experimental.pallas import tpu as pltpu
from jax.sharding import Mesh
from jax.sharding import PartitionSpec as P

TOP = 2
SPAN = 64
CHUNKS = (1,) * 15
WIDE_AT = (1, 6, -1, 2)
WIDE = 1
OUT_LAGS = (3, 6, 9)
BACK_LAGS = (3, 6, 8, 11)
AXES = ("ep_0", "ep_1", "ep_2", "tp")
EP = ("ep_0", "ep_1", "ep_2")
EP_TP = AXES
MESH = pl.DeviceIdType.MESH
epsilon = 1e-06
f32 = jnp.float32
bf16 = jnp.bfloat16


def dot(a, b):
    return jnp.dot(a, b, preferred_element_type=f32)


def dot_nt(a, b):
    return lax.dot_general(a, b, (((1,), (1,)), ((), ())), preferred_element_type=f32)


def dot_tn(a, b):
    return lax.dot_general(a, b, (((0,), (0,)), ((), ())), preferred_element_type=f32)


def regroup(outer, inner, slots):
    n = outer * inner * slots
    row = lax.broadcasted_iota(jnp.int32, (n, n), 0)
    col = lax.broadcasted_iota(jnp.int32, (n, n), 1)
    s_bits, i_bits = (slots - 1).bit_length(), (inner - 1).bit_length()
    o_bits = (outer - 1).bit_length()
    slot = row & (slots - 1)
    i = (row >> s_bits) & (inner - 1)
    o = row >> (s_bits + i_bits)
    source = (((i << o_bits) + o) << s_bits) + slot
    return jnp.where(col == source, 1.0, 0.0).astype(bf16)


def totals_rows(total):
    hi = total.astype(bf16).astype(f32)
    mid = (total - hi).astype(bf16).astype(f32)
    low = total - hi - mid
    rows = lax.broadcasted_iota(jnp.int32, (16, total.shape[1]), 0)
    return jnp.where(
        rows == 0, hi, jnp.where(rows == 1, mid, jnp.where(rows == 2, low, 0.0))
    ).astype(bf16)


def read_state(ref, index, rows):
    block = ref[index]
    return (
        block[:rows].astype(f32),
        jnp.sum(block[rows:].astype(f32), axis=0, keepdims=True),
    )


def chain(earlier, later):
    return (jnp.exp(later[1]) * earlier[0] + later[0], earlier[1] + later[1])


def keep_if(flag, new, old):
    return jax.tree.map(lambda a, b: jnp.where(flag, a, b), new, old)


def kernel(
    sizes,
    q_hbm, f_hbm, v_hbm, og_hbm, margin_ref, surge_ref, hgain_ref, x_hbm, egain_ref, routes_ref, logits_ref,
    wo_hbm, gate_hbm, up_hbm, down_hbm,
    mixed_ref, moe_ref,
    zs, zr, xs, arr, gate_v, up_v, down_v, wo_v, gacc, uacc, hb, ps, r1, r2, rx, xb, rzs, rzr,
    mp, m1, m2, s1, s2, s3, s4, s5, local_out, q_in, ha,
    tk, zsq, zrq, xsq, arrq, psq, xbq, rzsq, rzrq, uq, t1, t2, lg, q_send, q_recv,
    q_ref, f_ref, v_ref, og_ref, x_ref, in_sem, w_sem, z_send, z_recv, x_send, x_recv, y_send, y_recv,
    ra_send, rb_send, r_recv, rx_send, rx_recv, rz_send, rz_recv,
    m_send, m_recv, s_send, s_recv,
):
    Z, X, C, Y, widths = sizes
    NC = len(widths)
    starts = [sum(widths[:k]) for k in range(NC)]
    wide = slice(sum(widths), x_ref.shape[1])
    wq = x_ref.shape[1] - sum(widths)
    XC = X * C
    z, x, c, y = (lax.axis_index(a) for a in AXES)
    xc = x * C + c

    def of(ref, k, *index):
        index = (k,) + index
        rest = (slice(None),) * (len(ref.shape) - 1 - len(index))
        if widths[k] == ref.shape[-1]:
            return ref.at[index]
        return ref.at[index + rest + (pl.ds(0, widths[k]),)]

    def columns(k):
        return slice(starts[k], starts[k] + widths[k])

    heads, key = surge_ref.shape[0], s4.shape[2]
    seq = q_ref.shape[0]
    inputs = [
        pltpu.make_async_copy(src, dst, in_sem.at[i])
        for i, (src, dst) in enumerate(
            ((x_hbm, x_ref), (f_hbm, f_ref), (q_hbm, q_ref), (v_hbm, v_ref), (og_hbm, og_ref))
        )
    ]
    for copy in inputs:
        copy.start()
    quarter = s4.shape[1]
    up1, down1, across = lax.rem(y + 1, Y), lax.rem(y + Y - 1, Y), lax.rem(y + 2, Y)

    z_at = [lax.rem(z + d, Z) for d in range(Z)]
    xc_at = [lax.rem(xc + d, XC) for d in range(XC)]
    xc_at = [(j, j // C, lax.rem(j, C)) for j in xc_at]

    def remote(src, dst, send, recv, **at):
        return pltpu.make_async_remote_copy(
            src_ref=src,
            dst_ref=dst,
            send_sem=send,
            recv_sem=recv,
            device_id={**dict(zip(AXES, (z, x, c, y))), **at},
            device_id_type=MESH,
        )

    def await_bytes(ref, sem):
        pltpu.make_async_copy(ref, ref, sem).wait()

    def z_peers(body):
        for d in range(1, Z):
            body(z_at[d])

    def xc_peers(body):
        for d in range(1, XC):
            body(*xc_at[d])

    def x_peers(body):
        for d in range(1, X):
            body(lax.rem(x + d, X))

    barrier = pltpu.get_barrier_semaphore()

    def greet(**at):
        pl.semaphore_signal(
            barrier, inc=1, device_id={**dict(zip(AXES, (z, x, c, y))), **at}, device_id_type=MESH
        )

    z_peers(lambda k: greet(ep_0=k))
    xc_peers(lambda j, a, b: greet(ep_1=a, ep_2=b))
    greet(tp=up1)
    greet(tp=down1)

    weights = [
        pltpu.make_async_copy(src, dst, w_sem.at[i])
        for i, (src, dst) in enumerate(
            ((gate_hbm, gate_v), (up_hbm, up_v), (wo_hbm, wo_v), (down_hbm, down_v))
        )
    ]
    for copy in weights:
        copy.start()

    tokens = x_ref.shape[0]

    def tables(owner, logits):
        chosen = routes_ref[:, :tokens]
        for i in range(1, Y):
            chosen = jnp.where(owner == i, routes_ref[:, i * tokens : (i + 1) * tokens], chosen)
        return slot_tables(chosen, logits, Z * XC)

    owners = (y, down1, up1, across)
    place, comb = tables(y, logits_ref[...])
    inputs[0].wait()
    rows = x_ref[...].astype(f32)
    scale = lax.rsqrt(jnp.mean(rows * rows, axis=-1, keepdims=True) + epsilon)

    def fill(k):
        part = x_ref[:, columns(k)].astype(f32)
        normed = (part * scale * egain_ref[:, columns(k)]).astype(bf16)
        of(zs, k)[...] = dot(place, normed).astype(bf16).reshape(zs.shape[1:3] + (widths[k],))
        of(zr, k, z)[...] = of(zs, k, z)[...]

    def wide_0():
        part = x_ref[:, wide].astype(f32)
        tk[0] = (part * scale * egain_ref[:, wide]).astype(bf16).reshape(tk.shape[1:])
        remote(tk.at[0], tk.at[1], q_send.at[0], q_recv.at[0], tp=up1).start()
        remote(tk.at[0], tk.at[2], q_send.at[0], q_recv.at[1], tp=down1).start()
        remote(lg.at[0], lg.at[1], q_send.at[1], q_recv.at[4], tp=up1).start()
        remote(lg.at[0], lg.at[2], q_send.at[1], q_recv.at[5], tp=down1).start()

    def wide_1():
        for i, to in ((0, up1), (1, down1)):
            await_bytes(tk.at[1 + i], q_recv.at[i])
            remote(tk.at[1 + i, i], tk.at[3, i], q_send.at[0], q_recv.at[2 + i], tp=to).start()
        await_bytes(lg.at[1], q_recv.at[4])
        remote(lg.at[1], lg.at[3], q_send.at[1], q_recv.at[6], tp=up1).start()

    def wide_2():
        for i in range(2):
            await_bytes(tk.at[3, i], q_recv.at[2 + i])
        for rel in range(Y):
            put = place if rel == 0 else tables(owners[rel], logits_ref[...])[0]
            block = dot(put, tk[rel].reshape(-1, wq)).astype(bf16)
            zsq[:, rel] = block.reshape(Z, -1, wq)
        z_peers(lambda d: remote(zsq.at[d], zrq.at[z], q_send.at[2], q_recv.at[7], ep_0=d).start())
        zrq[z] = zsq[z]

    def wide_3():
        await_bytes(zrq.at[pl.ds(0, Z - 1)], q_recv.at[7])
        for rel in range(Y):
            block = dot(to_xc, zrq[:, rel].reshape(-1, wq)).astype(bf16)
            xsq[:, rel] = block.reshape(XC, -1, wq)
        xc_peers(
            lambda j, a, b: remote(
                xsq.at[j], arrq.at[:, xc], q_send.at[3], q_recv.at[8], ep_1=a, ep_2=b
            ).start()
        )
        arrq[:, xc] = xsq[xc]

    def wide_4():
        await_bytes(arrq.at[:, pl.ds(0, XC - 1)], q_recv.at[8])
        gathered = arrq[...].reshape(-1, wq)
        for acc, w in ((gacc, gate_v), (uacc, up_v)):
            acc[...] += dot_nt(gathered, w[:, wide])

    def wide_5():
        part = dot(hb[...], down_v[:, wide])
        psq[...] = part.astype(bf16).reshape(psq.shape)
        xc_peers(
            lambda j, a, b: remote(
                psq.at[:, j], xbq.at[xc], q_send.at[4], q_recv.at[9], ep_1=a, ep_2=b
            ).start()
        )
        xbq[xc] = psq[:, xc]

    def wide_6():
        await_bytes(xbq.at[pl.ds(0, XC - 1)], q_recv.at[9])
        for rel in range(Y):
            block = dot(to_z, xbq[:, rel].reshape(-1, wq)).astype(bf16)
            rzsq[:, rel] = block.reshape(Z, -1, wq)
        z_peers(
            lambda d: remote(rzsq.at[d], rzrq.at[z], q_send.at[5], q_recv.at[10], ep_0=d).start()
        )
        rzrq[z] = rzsq[z]

    def weighed(table, results):
        table = table.T
        hi = table.astype(bf16)
        low = (table - hi.astype(f32)).astype(bf16)
        return dot(hi, results) + dot(low, results)

    def wide_7():
        await_bytes(rzrq.at[pl.ds(0, Z - 1)], q_recv.at[10])
        await_bytes(lg.at[2], q_recv.at[5])
        await_bytes(lg.at[3], q_recv.at[6])
        for rel in range(Y):
            table = tables(owners[rel], lg[rel][:TOP, :tokens])[1]
            part = weighed(table, rzrq[:, rel].reshape(-1, wq))
            uq[rel] = part.astype(bf16).reshape(uq.shape[1:])
        for i, to in ((0, up1), (1, down1)):
            remote(uq.at[3, i], t1.at[i], q_send.at[6], q_recv.at[11 + i], tp=to).start()

    def wide_8():
        for i, rel, to in ((0, 2, up1), (1, 1, down1)):
            await_bytes(t1.at[i], q_recv.at[11 + i])
            uq[rel, i] = (uq[rel, i].astype(f32) + t1[i].astype(f32)).astype(bf16)
            remote(uq.at[rel], t2.at[i], q_send.at[7], q_recv.at[13 + i], tp=to).start()

    def wide_9():
        await_bytes(t2.at[0], q_recv.at[13])
        await_bytes(t2.at[1], q_recv.at[14])
        total = uq[0].astype(f32) + t2[0].astype(f32) + t2[1].astype(f32)
        moe_ref[:, wide] = total.astype(bf16).reshape(tokens, wq)

    lg[0] = jnp.zeros(lg.shape[1:], f32)
    lg[0, :TOP, :tokens] = logits_ref[...]

    def z_go(k):
        z_peers(
            lambda d: remote(
                of(zs, k, d), of(zr, k, z), z_send.at[k], z_recv.at[k], ep_0=d
            ).start()
        )

    for k in range(NC):
        fill(k)
        if k == 0:
            pl.semaphore_wait(barrier, Z - 1 + XC - 1 + 2)
        z_go(k)
        if k == 0:
            wide_0()

    to_xc = regroup(XC, Z, 2)
    to_z = regroup(Z, XC, 2)

    def step_a(k):
        await_bytes(of(zr, k, pl.ds(0, Z - 1)), z_recv.at[k])
        block = dot(to_xc, of(zr, k)[...].reshape(-1, widths[k])).astype(bf16)
        of(xs, k)[...] = block.reshape(xs.shape[1:3] + (widths[k],))
        xc_peers(
            lambda j, a, b: remote(
                of(xs, k, j), of(arr, k, 0, xc), x_send.at[k], x_recv.at[k], ep_1=a, ep_2=b
            ).start()
        )
        of(arr, k, 0, xc)[...] = of(xs, k, xc)[...]

    def step_b(k):
        await_bytes(of(arr, k, 0, pl.ds(0, XC - 1)), x_recv.at[k])
        remote(of(arr, k, 0), of(arr, k, 1), y_send.at[k], y_recv.at[k, 0], tp=up1).start()
        remote(of(arr, k, 0), of(arr, k, 2), y_send.at[k], y_recv.at[k, 1], tp=down1).start()

    half = XC // 2

    def step_c(k):
        await_bytes(of(arr, k, 1), y_recv.at[k, 0])
        low = pl.ds(0, half)
        remote(
            of(arr, k, 1, low), of(arr, k, 3, low), y_send.at[k], y_recv.at[k, 2], tp=up1
        ).start()
        await_bytes(of(arr, k, 2), y_recv.at[k, 1])
        high = pl.ds(half, half)
        remote(
            of(arr, k, 2, high), of(arr, k, 3, high), y_send.at[k], y_recv.at[k, 3], tp=down1
        ).start()

    def step_d(k):
        await_bytes(of(arr, k, 3, pl.ds(0, half)), y_recv.at[k, 2])
        await_bytes(of(arr, k, 3, pl.ds(half, half)), y_recv.at[k, 3])
        if k == 0:
            weights[0].wait()
            weights[1].wait()
        tokens = of(arr, k)[...].reshape(-1, widths[k])
        for acc, w in ((gacc, gate_v), (uacc, up_v)):
            part = dot_nt(tokens, w[:, columns(k)])
            if k == 0:
                acc[...] = part
            elif k < NC - 1:
                acc[...] += part
            elif acc is gacc:
                gate = acc[...] + part
            else:
                hb[...] = (jax.nn.silu(gate) * (acc[...] + part)).astype(bf16)

    def recurrence():
        for copy in inputs[1:4]:
            copy.wait()
        shut = jax.nn.sigmoid(-f_ref[...].astype(f32)) * margin_ref[...]
        tri = jnp.where(
            lax.broadcasted_iota(jnp.int32, (seq, seq), 0)
            >= lax.broadcasted_iota(jnp.int32, (seq, seq), 1),
            1.0,
            0.0,
        )
        highest = lax.Precision.HIGHEST
        run_all = jnp.dot(tri, jnp.log1p(-shut), precision=highest, preferred_element_type=f32)
        surges = lax.dot_general(
            tri, surge_ref[...], (((1,), (1,)), ((), ())), precision=highest, preferred_element_type=f32
        )
        causal = lax.broadcasted_iota(jnp.int32, (SPAN, SPAN), 0) >= lax.broadcasted_iota(
            jnp.int32, (SPAN, SPAN), 1
        )
        for h in range(heads):
            cols = slice(h * key, (h + 1) * key)
            run = run_all[:, cols] + surges[:, h : h + 1]
            query = q_ref[:, cols].astype(f32)
            inflow = shut[:, cols]
            value = v_ref[:, cols]
            q_in[h] = (query * jnp.exp(run)).astype(bf16)
            state = None
            for i in range(seq // SPAN):
                at = slice(i * SPAN, (i + 1) * SPAN)
                r, qs, ks, vs = run[at], query[at], inflow[at], value[at]
                mid = r[SPAN // 2 : SPAN // 2 + 1]
                lifted = (qs * jnp.exp(r - mid)).astype(bf16)
                lowered = (ks * jnp.exp(mid - r)).astype(bf16)
                scores = jnp.where(causal, dot_nt(lifted, lowered), 0.0)
                out = dot(scores.astype(bf16), vs)
                close = r[SPAN - 1 : SPAN]
                added = dot_tn(vs, (ks * jnp.exp(close - r)).astype(bf16))
                if state is None:
                    state = added
                else:
                    before = run[i * SPAN - 1 : i * SPAN]
                    out = out + dot_nt((qs * jnp.exp(r - before)).astype(bf16), state.astype(bf16))
                    state = jnp.exp(close - before) * state + added
                local_out[at, cols] = out
            s1[c, h, pl.ds(0, key)] = state.astype(bf16)
            s1[c, h, pl.ds(key, 16)] = totals_rows(run[seq - 1 : seq])
        remote(s1.at[c], s1.at[c], s_send.at[0], s_recv.at[0], ep_2=1 - c).start()

    empty = lambda n: (jnp.zeros((n, key), f32), jnp.zeros((1, key), f32))

    def state_2():
        await_bytes(s1.at[1 - c], s_recv.at[0])
        both = chain(read_state(s1, (0, c), key), read_state(s1, (1, c), key))
        s2[x, pl.ds(0, key)] = both[0].astype(bf16)
        s2[x, pl.ds(key, 16)] = totals_rows(both[1])
        x_peers(
            lambda a: remote(s2.at[x], s2.at[x], s_send.at[1], s_recv.at[1], ep_1=a).start()
        )

    def x_prefix():
        prefix = empty(key)
        total = empty(key)
        for i in range(X):
            total = chain(total, read_state(s2, (i,), key))
            if i < X - 1:
                prefix = keep_if(i + 1 == x, total, prefix)
        return prefix, total

    def state_3():
        await_bytes(s2.at[pl.ds(0, X - 1)], s_recv.at[1])
        _, total = x_prefix()
        mine = total[0][:quarter]
        for i in range(1, X):
            mine = jnp.where(x == i, total[0][i * quarter : (i + 1) * quarter], mine)
        s3[z, pl.ds(0, quarter)] = mine.astype(bf16)
        s3[z, pl.ds(quarter, 16)] = totals_rows(total[1])
        z_peers(
            lambda k: remote(s3.at[z], s3.at[z], s_send.at[2], s_recv.at[2], ep_0=k).start()
        )

    def state_4():
        await_bytes(s3.at[pl.ds(0, Z - 1)], s_recv.at[2])
        prefix = empty(quarter)
        total = empty(quarter)
        for i in range(Z - 1):
            total = chain(total, read_state(s3, (i,), quarter))
            prefix = keep_if(i + 1 == z, total, prefix)
        s4[x] = prefix[0].astype(bf16)
        x_peers(
            lambda a: remote(s4.at[x], s4.at[x], s_send.at[3], s_recv.at[3], ep_1=a).start()
        )

    def state_5():
        await_bytes(s4.at[pl.ds(0, X - 1)], s_recv.at[3])
        before = s4[...].astype(f32).reshape(key, key)
        prefix, _ = x_prefix()
        s5[c] = (jnp.exp(prefix[1]) * before + prefix[0]).astype(bf16)
        remote(s5.at[c], s5.at[c], s_send.at[4], s_recv.at[4], ep_2=1 - c).start()

    def mix():
        inputs[4].wait()
        await_bytes(s5.at[1 - c], s_recv.at[4])
        for h in range(heads):
            cols = slice(h * key, (h + 1) * key)
            chip = s5[h].astype(f32)
            first = read_state(s1, (0, h), key)
            entering = jnp.where(c == 0, chip, jnp.exp(first[1]) * chip + first[0])
            out = local_out[:, cols] + dot_nt(q_in[h], entering.astype(bf16))
            out = out * lax.rsqrt(jnp.mean(out * out, axis=-1, keepdims=True) + epsilon)
            gate = og_ref[:, cols].astype(f32)
            ha[:, cols] = (out * hgain_ref[:, cols] * jax.nn.silu(gate)).astype(bf16)
        weights[2].wait()
        for at in [columns(k) for k in range(NC)] + [wide]:
            part = dot(ha[...], wo_v[:, at]).astype(bf16)
            mp[:, :, :, at] = part.reshape(mp.shape[:3] + (at.stop - at.start,))

    def mix_a():
        remote(mp.at[across, 0], m1.at[0], m_send.at[0], m_recv.at[0], tp=up1).start()
        remote(mp.at[across, 1], m1.at[1], m_send.at[0], m_recv.at[1], tp=down1).start()

    def mix_b():
        for i, to in ((0, up1), (1, down1)):
            await_bytes(m1.at[i], m_recv.at[i])
            mp[to, i] = (mp[to, i].astype(f32) + m1[i].astype(f32)).astype(bf16)
            remote(mp.at[to], m2.at[i], m_send.at[1], m_recv.at[2 + i], tp=to).start()

    def mix_c():
        await_bytes(m2.at[0], m_recv.at[2])
        await_bytes(m2.at[1], m_recv.at[3])
        total = mp[y].astype(f32) + m2[0].astype(f32) + m2[1].astype(f32)
        mixed_ref[...] = total.astype(bf16).reshape(mixed_ref.shape)

    def step_e(k):
        if k == 0:
            weights[3].wait()
        part = dot(hb[...], down_v[:, columns(k)])
        of(ps, k)[...] = part.astype(bf16).reshape(ps.shape[1:4] + (widths[k],))
        for i, to in ((0, up1), (1, down1)):
            remote(of(ps, k, 3, i), of(r1, k, i), ra_send.at[k], r_recv.at[k, i], tp=to).start()

    def step_f(k):
        for i, rel, to in ((0, 2, up1), (1, 1, down1)):
            await_bytes(of(r1, k, i), r_recv.at[k, i])
            mine = of(ps, k, rel, i)
            mine[...] = (mine[...].astype(f32) + of(r1, k, i)[...].astype(f32)).astype(bf16)
            remote(
                of(ps, k, rel), of(r2, k, i), rb_send.at[k], r_recv.at[k, 2 + i], tp=to
            ).start()

    def step_g(k):
        await_bytes(of(r2, k, 0), r_recv.at[k, 2])
        await_bytes(of(r2, k, 1), r_recv.at[k, 3])
        total = of(ps, k, 0)[...].astype(f32)
        for i in range(2):
            total = total + of(r2, k, i)[...].astype(f32)
        of(rx, k)[...] = total.astype(bf16).reshape(rx.shape[1:3] + (widths[k],))
        xc_peers(
            lambda j, a, b: remote(
                of(rx, k, j), of(xb, k, xc), rx_send.at[k], rx_recv.at[k], ep_1=a, ep_2=b
            ).start()
        )
        of(xb, k, xc)[...] = of(rx, k, xc)[...]

    def step_h(k):
        await_bytes(of(xb, k, pl.ds(0, XC - 1)), rx_recv.at[k])
        block = dot(to_z, of(xb, k)[...].reshape(-1, widths[k])).astype(bf16)
        of(rzs, k)[...] = block.reshape(rzs.shape[1:3] + (widths[k],))
        z_peers(
            lambda d: remote(
                of(rzs, k, d), of(rzr, k, z), rz_send.at[k], rz_recv.at[k], ep_0=d
            ).start()
        )
        of(rzr, k, z)[...] = of(rzs, k, z)[...]

    comb = comb.T
    comb_hi = comb.astype(bf16)
    comb_lo = (comb - comb_hi.astype(f32)).astype(bf16)

    def step_i(k):
        await_bytes(of(rzr, k, pl.ds(0, Z - 1)), rz_recv.at[k])
        results = of(rzr, k)[...].reshape(-1, widths[k])
        moe_ref[:, columns(k)] = (dot(comb_hi, results) + dot(comb_lo, results)).astype(bf16)

    recurrence()
    wide_1()
    lag_b, lag_c, lag_d = OUT_LAGS
    for t in range(NC + lag_d):
        if t < NC:
            step_a(t)
        if t == NC + 1:
            mix()
        if 0 <= t - lag_b < NC:
            step_b(t - lag_b)
        if 0 <= t - lag_c < NC:
            step_c(t - lag_c)
        if t - lag_c == NC - 1:
            mix_a()
        if t == 0:
            state_2()
        if t == 1:
            state_3()
            wide_2()
        if t == NC + WIDE_AT[0]:
            wide_3()
        if t - lag_d == NC - 1:
            wide_4()
        if t == NC:
            state_4()
        if 0 <= t - lag_d < NC:
            step_d(t - lag_d)
        if t == NC:
            state_5()
    lag_f, lag_g, lag_h, lag_i = BACK_LAGS
    for t in range(NC + lag_i):
        if t < NC:
            step_e(t)
        if t == 1:
            wide_5()
        if t == WIDE_AT[1]:
            wide_6()
        if t == NC + WIDE_AT[2]:
            wide_7()
        if 0 <= t - lag_f < NC:
            step_f(t - lag_f)
        if t - lag_f == NC - 1:
            mix_b()
        if t == NC + WIDE_AT[3]:
            wide_8()
        if 0 <= t - lag_g < NC:
            step_g(t - lag_g)
        if 0 <= t - lag_h < NC:
            step_h(t - lag_h)
        if t - lag_i == NC - 1:
            mix_c()
            wide_9()
        if 0 <= t - lag_i < NC:
            step_i(t - lag_i)

    for k in range(NC):
        await_bytes(of(zs, k, pl.ds(0, Z - 1)), z_send.at[k])
        await_bytes(of(xs, k, pl.ds(0, XC - 1)), x_send.at[k])
        await_bytes(of(arr, k, pl.ds(0, 3)), y_send.at[k])
        await_bytes(of(ps, k, 3), ra_send.at[k])
        await_bytes(of(ps, k, pl.ds(1, 2)), rb_send.at[k])
        await_bytes(of(rx, k, pl.ds(0, XC - 1)), rx_send.at[k])
        await_bytes(of(rzs, k, pl.ds(0, Z - 1)), rz_send.at[k])
    await_bytes(mp.at[0], m_send.at[0])
    await_bytes(mp.at[pl.ds(0, 2)], m_send.at[1])
    await_bytes(s1.at[0], s_send.at[0])
    await_bytes(s2.at[pl.ds(0, X - 1)], s_send.at[1])
    await_bytes(s3.at[pl.ds(0, Z - 1)], s_send.at[2])
    await_bytes(s4.at[pl.ds(0, X - 1)], s_send.at[3])
    await_bytes(s5.at[0], s_send.at[4])
    await_bytes(tk.at[pl.ds(0, 3)], q_send.at[0])
    await_bytes(lg.at[pl.ds(0, 3)], q_send.at[1])
    await_bytes(zsq.at[pl.ds(0, Z - 1)], q_send.at[2])
    await_bytes(xsq.at[pl.ds(0, XC - 1)], q_send.at[3])
    await_bytes(psq.at[:, pl.ds(0, XC - 1)], q_send.at[4])
    await_bytes(rzsq.at[pl.ds(0, Z - 1)], q_send.at[5])
    await_bytes(uq.at[3], q_send.at[6])
    await_bytes(uq.at[pl.ds(1, 2)], q_send.at[7])


def slot_tables(chosen, logits, experts):
    tokens = chosen.shape[1]
    top = jnp.max(logits, axis=0, keepdims=True)
    raised = jnp.exp(logits - top)
    weight = raised / jnp.sum(raised, axis=0, keepdims=True)
    expert = lax.broadcasted_iota(jnp.int32, (experts, tokens), 0)
    named = [jnp.where(expert == chosen[j : j + 1], 1.0, 0.0) for j in range(TOP)]
    earlier = lax.broadcasted_iota(jnp.int32, (tokens, tokens), 0) < lax.broadcasted_iota(
        jnp.int32, (tokens, tokens), 1
    )
    before = dot(sum(named).astype(bf16), jnp.where(earlier, 1.0, 0.0).astype(bf16))
    row = lax.broadcasted_iota(jnp.int32, (2 * experts, tokens), 0).astype(f32)
    place = jnp.zeros((2 * experts, tokens), f32)
    comb = place
    for j in range(TOP):
        rank = jnp.sum(named[j] * before, axis=0, keepdims=True)
        here = row == 2.0 * chosen[j : j + 1].astype(f32) + rank
        place = jnp.where(here, 1.0, place)
        comb = jnp.where(here, weight[j : j + 1], comb)
    return place.astype(bf16), comb


def hand_on(mixed_in, moe_in, mixed_out, moe_out):
    mixed_out[...] = mixed_in[...]
    moe_out[...] = moe_in[...]


def per_device(
    sizes,
    recurrence_query,
    forget_preactivation,
    recurrence_value,
    output_gate_preactivation,
    forget_margin,
    surge_log_decay,
    head_norm_gain,
    recurrence_output_matrix,
    second_micro_input,
    expert_norm_gain,
    routes,
    router_chosen_logits,
    expert_gate_matrix,
    expert_up_matrix,
    expert_down_matrix,
):
    Z, X, C, Y, shares = sizes
    NC = len(shares)
    XC = X * C
    experts = Z * XC
    tokens, D = second_micro_input.shape
    seq, width = recurrence_query.shape
    heads = surge_log_decay.shape[0]
    key = width // heads
    F = expert_gate_matrix.shape[2]
    widths = tuple(D * share // (sum(shares) + WIDE) for share in shares)
    wq = D - sum(widths)
    W = max(widths)
    slots = 2 * experts
    V = pltpu.VMEM
    DMA = pltpu.SemaphoreType.DMA
    scratch = [
        V((NC, Z, 2 * XC, W), bf16),
        V((NC, Z, 2 * XC, W), bf16),
        V((NC, XC, 2 * Z, W), bf16),
        V((NC, Y, XC, 2 * Z, W), bf16),
        V((F, D), bf16),
        V((F, D), bf16),
        V((F, D), bf16),
        V((width, D), bf16),
        V((Y * slots, F), f32),
        V((Y * slots, F), f32),
        V((Y * slots, F), bf16),
        V((NC, Y, 2, slots // 2, W), bf16),
        V((NC, 2, slots // 2, W), bf16),
        V((NC, 2, 2, slots // 2, W), bf16),
        V((NC, XC, 2 * Z, W), bf16),
        V((NC, XC, 2 * Z, W), bf16),
        V((NC, Z, 2 * XC, W), bf16),
        V((NC, Z, 2 * XC, W), bf16),
        V((Y, 2, seq // Y // 2, D), bf16),
        V((2, seq // Y // 2, D), bf16),
        V((2, 2, seq // Y // 2, D), bf16),
        V((C, heads, key + 16, key), bf16),
        V((X, key + 16, key), bf16),
        V((Z, key // X + 16, key), bf16),
        V((X, key // X, key), bf16),
        V((C, key, key), bf16),
        V((seq, width), f32),
        V((heads, seq, key), bf16),
        V((seq, width), bf16),
        V((Y, 2, tokens // 2, wq), bf16),
        V((Z, Y, 2 * XC, wq), bf16),
        V((Z, Y, 2 * XC, wq), bf16),
        V((XC, Y, 2 * Z, wq), bf16),
        V((Y, XC, 2 * Z, wq), bf16),
        V((Y, XC, 2 * Z, wq), bf16),
        V((XC, Y, 2 * Z, wq), bf16),
        V((Z, Y, 2 * XC, wq), bf16),
        V((Z, Y, 2 * XC, wq), bf16),
        V((Y, 2, tokens // 2, wq), bf16),
        V((2, tokens // 2, wq), bf16),
        V((2, 2, tokens // 2, wq), bf16),
        V((Y, 8, 128), f32),
        DMA((8,)),
        DMA((15,)),
        V((seq, width), bf16),
        V((seq, width), bf16),
        V((seq, width), bf16),
        V((seq, width), bf16),
        V((tokens, D), bf16),
        DMA((5,)),
        DMA((4,)),
        DMA((NC,)),
        DMA((NC,)),
        DMA((NC,)),
        DMA((NC,)),
        DMA((NC,)),
        DMA((NC, 4)),
        DMA((NC,)),
        DMA((NC,)),
        DMA((NC, 4)),
        DMA((NC,)),
        DMA((NC,)),
        DMA((NC,)),
        DMA((NC,)),
        DMA((2,)),
        DMA((4,)),
        DMA((5,)),
        DMA((5,)),
    ]
    vmem = pl.BlockSpec(memory_space=pltpu.VMEM)
    hbm = pl.BlockSpec(memory_space=pl.ANY)
    out = jax.ShapeDtypeStruct((tokens, D), bf16)
    results = pl.pallas_call(
        functools.partial(kernel, sizes[:4] + (widths,)),
        out_shape=(jax.ShapeDtypeStruct((seq // Y, D), bf16), out),
        in_specs=[hbm] * 4 + [vmem] * 3 + [hbm] + [vmem] * 3 + [hbm] * 4,
        out_specs=(vmem, vmem),
        scratch_shapes=scratch,
        compiler_params=pltpu.CompilerParams(
            collective_id=0, has_side_effects=True, vmem_limit_bytes=63 * 1024 * 1024
        ),
    )(
        recurrence_query,
        forget_preactivation,
        recurrence_value,
        output_gate_preactivation,
        forget_margin.reshape(1, -1),
        surge_log_decay,
        head_norm_gain.reshape(1, -1),
        second_micro_input,
        expert_norm_gain.reshape(1, -1),
        routes.T,
        router_chosen_logits.T,
        recurrence_output_matrix,
        expert_gate_matrix[0].T,
        expert_up_matrix[0].T,
        expert_down_matrix[0],
    )
    return pl.pallas_call(
        hand_on,
        out_shape=(jax.ShapeDtypeStruct((seq // Y, D), bf16), out),
        in_specs=[vmem] * 2,
        out_specs=(vmem, vmem),
    )(*results)


def build(finer, chunks):
    sizes = tuple(finer.shape[a] for a in AXES) + (chunks,)
    in_specs = (
        P(EP, "tp"),
        P(EP, "tp"),
        P(EP, "tp"),
        P(EP, "tp"),
        P("tp"),
        P("tp", EP),
        P("tp"),
        P("tp", None),
        P(EP_TP, None),
        P(),
        P(EP, None),
        P(EP_TP, None),
        P(EP, None, "tp"),
        P(EP, None, "tp"),
        P(EP, "tp", None),
    )
    out_specs = (P(EP_TP, None), P(EP_TP, None))
    return jax.shard_map(
        functools.partial(per_device, sizes),
        mesh=finer,
        in_specs=in_specs,
        out_specs=out_specs,
        check_vma=False,
    )


def solution(mesh):
    return build(Mesh(mesh.devices.reshape(8, 4, 2, mesh.shape["tp"]), AXES), CHUNKS)
```
